128 devices in a mesh: sp: 16 (over z, x), tp: 8 (over y, core).
Axes of the slice: x: 4, y: 4, z: 4, core: 2. Of those that a mesh axis runs over, the one named last changes fastest.
Arguments:
- prompt: bfloat16 [4, 8192, 4096], P(None, 'sp'), may hold values from -6 to 6
- key_weight: bfloat16 [4096, 1024], P(None, 'tp'), may hold values from -0.09375 to 0.09375
- value_weight: bfloat16 [4096, 2048], P(None, 'tp'), may hold values from -0.09375 to 0.09375
- input_gate_weight: bfloat16 [4096, 16], P(None, 'tp'), may hold values from -0.09375 to 0.09375
- forget_gate_weight: bfloat16 [4096, 16], P(None, 'tp'), may hold values from -0.09375 to 0.09375
- forget_bias: float32 [16], P('tp'), may hold values from 3 to 11
- key_taps: bfloat16 [3, 1024], P(None, 'tp'), may hold values from -3 to 3
- extra_decay: float32 [4, 8192, 16], P(None, 'sp', 'tp'), may hold values from -1.5 to 0
- new_query: bfloat16 [4, 16, 64], P(None, 'tp'), may hold values from -6 to 6
- new_key: bfloat16 [4, 16, 64], P(None, 'tp'), may hold values from -6 to 6
- new_value: bfloat16 [4, 16, 128], P(None, 'tp', 'sp'), may hold values from -6 to 6
- new_input_gate: float32 [4, 16], P(None, 'tp'), may hold values from 2 to 7
- new_forget_gate: float32 [4, 16], P(None, 'tp'), may hold values from -2 to 4
- out_weight: bfloat16 [16, 128, 4096], P('tp', 'sp'), may hold values from -0.125 to 0.125
Outputs:
- cache_memory: bfloat16 [4, 16, 64, 128], P(None, 'tp', None, 'sp')
- cache_norm: bfloat16 [4, 16, 64], P(None, 'tp', 'sp')
- cache_peak: float32 [4, 16], P(None, 'tp')
- read_out: bfloat16 [4, 4096], P(None, ('sp', 'tp'))
The draws below stay inside these ranges and needn't reach their ends.
All inputs are finite; a program needn't handle non-finite values.
Results may differ from the reference program's by a relative error of at most 0.012.
The reference program's roundings to bfloat16 on the way count: a program that leaves them out, or rounds other values in their place, can miss the bound.
Values may be sent and summed in bfloat16 or wider, within the bound.
No kernel may reach another device: no remote copies, remote signals or barrier semaphores. Data moves between devices by JAX's collectives and lax.ppermute only.
A program may use at most 64 MiB of HBM per device.

```python
import math
import jax
import jax.numpy as jnp
from jax import lax

D = 4096
HEAD_TOTAL = 16
KEY_DIM = 64
VALUE_DIM = 128
TAPS = 3
PROMPT_COUNT = 4
SEG = 512
PROMPT_LENGTH = 8192


def draw_forget_bias(key, part):
    first_key, second_key, third_key = jax.random.split(key, 3)
    chooser = jax.random.uniform(first_key, (HEAD_TOTAL,), jnp.float32)
    share = 0.5
    quick_bias = jax.random.uniform(second_key, (HEAD_TOTAL,), jnp.float32, 3.0, 4.2)
    steady_bias = jnp.log(jnp.float32(PROMPT_LENGTH)) + jax.random.uniform(third_key, (HEAD_TOTAL,), jnp.float32, 1.5, 3.0)
    steady_bias = jnp.minimum(steady_bias, 11.0)
    return jnp.where(chooser < share, quick_bias, steady_bias)


def draw_extra_decay(key, part):
    key_seg, key_location, key_depth = jax.random.split(key, 3)
    blocks = PROMPT_LENGTH // SEG
    seg_log = jax.random.uniform(key_seg, (PROMPT_COUNT, blocks, HEAD_TOTAL), jnp.float32, math.log(0.005), math.log(0.05))
    stable_offset = jnp.repeat(-jnp.exp(seg_log) / SEG, SEG, axis=1)
    spike_location = jax.random.randint(key_location, (PROMPT_COUNT, 2, HEAD_TOTAL), 0, PROMPT_LENGTH)
    depth_limit = jax.random.uniform(key_depth, (PROMPT_COUNT, 2, HEAD_TOTAL), jnp.float32, 0.22, 0.7)
    token_position = jnp.arange(PROMPT_LENGTH)
    hit_values = token_position[None, :, None, None] == spike_location[:, None, :, :]
    spike_values = jnp.sum(jnp.where(hit_values, -depth_limit[:, None, :, :], 0.0), axis=2)
    return stable_offset + spike_values


def levels(key, dims, pieces, smallest, top_value):
    gain = 1.0
    for dim, parts in pieces:
        draws = jax.random.uniform(jax.random.fold_in(jax.random.fold_in(key, 6), dim), (parts,), jnp.float32, smallest / len(pieces), top_value / len(pieces))
        gain = gain * jnp.repeat(jnp.exp(draws), dims[dim] // parts).reshape((-1,) + (1,) * (len(dims) - 1 - dim))
    return gain


def scatter_about(own_key, shape, width, limit, shards=(), held_as=jnp.bfloat16):
    level = levels(own_key, shape, shards, -0.22, 0.18) if shards else 1.0
    drawn = jax.random.normal(own_key, shape, jnp.float32) * width * level
    return jnp.minimum(jnp.maximum(drawn, -limit), limit).astype(held_as)


def setup_inputs(seed: int = 0) -> dict:
    seeds = jax.random.split(jax.random.key(seed), 15)
    prompt = scatter_about(seeds[0], (PROMPT_COUNT, PROMPT_LENGTH, D), 1.0, 6.0, ((1, 16),))
    key_weight = scatter_about(seeds[1], (D, HEAD_TOTAL * KEY_DIM), D ** -0.5, 0.09375, ((1, 8),))
    value_weight = scatter_about(seeds[2], (D, HEAD_TOTAL * VALUE_DIM), D ** -0.5, 0.09375, ((1, 8),))
    input_gate_weight = scatter_about(seeds[3], (D, HEAD_TOTAL), D ** -0.5, 0.09375, ((1, 8),))
    forget_gate_weight = scatter_about(seeds[4], (D, HEAD_TOTAL), D ** -0.5, 0.09375, ((1, 8),))
    forget_bias = draw_forget_bias(jax.random.fold_in(seeds[14], 71), 0)
    key_taps = scatter_about(seeds[6], (TAPS, HEAD_TOTAL * KEY_DIM), 0.577, 3.0, ((1, 8),))
    extra_decay = draw_extra_decay(jax.random.fold_in(seeds[14], 71), 0)
    new_query = scatter_about(seeds[8], (PROMPT_COUNT, HEAD_TOTAL, KEY_DIM), 1.0, 6.0, ((1, 8),))
    new_key = scatter_about(seeds[9], (PROMPT_COUNT, HEAD_TOTAL, KEY_DIM), 1.0, 6.0, ((1, 8),))
    new_value = scatter_about(seeds[10], (PROMPT_COUNT, HEAD_TOTAL, VALUE_DIM), 1.0, 6.0, ((1, 8), (2, 16)))
    new_input_gate = jnp.clip(2.0 + 5.0 * jax.random.uniform(seeds[11], (PROMPT_COUNT, HEAD_TOTAL), jnp.float32) ** levels(seeds[11], (PROMPT_COUNT, HEAD_TOTAL), ((1, 8),), -0.2, 0.2), 2.0, 7.0)
    new_forget_gate = jnp.clip(-2.0 + 6.0 * jax.random.uniform(seeds[12], (PROMPT_COUNT, HEAD_TOTAL), jnp.float32) ** levels(seeds[12], (PROMPT_COUNT, HEAD_TOTAL), ((1, 8),), -0.2, 0.2), -2.0, 4.0)
    out_weight = scatter_about(seeds[13], (HEAD_TOTAL, VALUE_DIM, D), (HEAD_TOTAL * VALUE_DIM) ** -0.5, 0.125, ((0, 8), (1, 16)))
    return dict(prompt=prompt, key_weight=key_weight, value_weight=value_weight, input_gate_weight=input_gate_weight, forget_gate_weight=forget_gate_weight, forget_bias=forget_bias, key_taps=key_taps, extra_decay=extra_decay, new_query=new_query, new_key=new_key, new_value=new_value, new_input_gate=new_input_gate, new_forget_gate=new_forget_gate, out_weight=out_weight)


def widen(rounded):
    return lax.optimization_barrier(rounded).astype(jnp.float32)


def key_conv(key_raw, key_taps):
    padded = jnp.pad(key_raw, ((1, 1), (0, 0)))
    tap_f32 = key_taps.astype(jnp.float32)
    mixed = tap_f32[0] * padded[:-2] + tap_f32[1] * padded[1:-1] + tap_f32[2] * padded[2:]
    return (jax.nn.silu(mixed) * KEY_DIM ** -0.5).astype(jnp.bfloat16)


def reference(prompt, key_weight, value_weight, input_gate_weight, forget_gate_weight, forget_bias,
              key_taps, extra_decay, new_query, new_key, new_value, new_input_gate, new_forget_gate,
              out_weight):
    def prompt_state(inputs):
        seq_rows, seq_extra = inputs
        key_raw = jnp.dot(seq_rows, key_weight, preferred_element_type=jnp.float32).astype(jnp.bfloat16)
        values = jnp.dot(seq_rows, value_weight, preferred_element_type=jnp.float32).astype(jnp.bfloat16)
        input_pre = widen(jnp.dot(seq_rows, input_gate_weight, preferred_element_type=jnp.float32).astype(jnp.bfloat16))
        forget_pre = widen(jnp.dot(seq_rows, forget_gate_weight, preferred_element_type=jnp.float32).astype(jnp.bfloat16))
        key_rows = key_conv(key_raw, key_taps)
        log_forget = jax.nn.log_sigmoid(forget_pre + forget_bias) + seq_extra
        suffix = jnp.sum(log_forget, axis=0, keepdims=True) - jnp.cumsum(log_forget, axis=0)
        gate_log = input_pre + suffix
        peak_log = jnp.max(gate_log, axis=0)
        scale = jnp.exp(gate_log - peak_log[None])
        key_quartet = key_rows.reshape(PROMPT_LENGTH, HEAD_TOTAL, KEY_DIM).astype(jnp.float32)
        value_four = values.reshape(PROMPT_LENGTH, HEAD_TOTAL, VALUE_DIM)
        weighted_rows = (value_four * scale[:, :, None]).astype(jnp.bfloat16)
        memory_matrix = jnp.einsum('xje,xjb->jeb', key_quartet, weighted_rows.astype(jnp.float32))
        normer = jnp.einsum('lh,lhk->hk', scale, key_quartet, precision=lax.Precision.HIGHEST)
        return memory_matrix, normer, peak_log

    memory_matrix, normer, peak_log = lax.map(prompt_state, (prompt, extra_decay))
    forget_new = jax.nn.log_sigmoid(new_forget_gate)
    new_peak = jnp.maximum(forget_new + peak_log, new_input_gate)
    old_scale = jnp.exp(forget_new + peak_log - new_peak)
    new_scale = jnp.exp(new_input_gate - new_peak)
    key_new = new_key.astype(jnp.float32)
    value_new = new_value.astype(jnp.float32)
    memory_next = (old_scale[:, :, None, None] * memory_matrix
                   + new_scale[:, :, None, None] * key_new[:, :, :, None] * value_new[:, :, None, :])
    normer_next = old_scale[:, :, None] * normer + new_scale[:, :, None] * key_new
    query = new_query.astype(jnp.float32)
    numer = jnp.sum(query[:, :, :, None] * memory_next, axis=2)
    denom = jnp.sum(query * normer_next, axis=-1)
    read = (numer / jnp.maximum(jnp.abs(denom), 1.0)[:, :, None]).astype(jnp.bfloat16)
    read_out = jnp.dot(read.reshape(PROMPT_COUNT, HEAD_TOTAL * VALUE_DIM), out_weight.reshape(HEAD_TOTAL * VALUE_DIM, D),
                       preferred_element_type=jnp.float32).astype(jnp.bfloat16)
    return memory_matrix.astype(jnp.bfloat16), normer.astype(jnp.bfloat16), peak_log, read_out
```

```python
import jax
import jax.numpy as jnp
from jax import lax
from jax.experimental import pallas as pl
from jax.experimental.pallas import tpu as pltpu
from jax.sharding import Mesh
from jax.sharding import PartitionSpec as P

KEY_DIM = 64
SP = ("sp_0", "sp_1")
SP_TP = ("sp_0", "sp_1", "tp_0", "tp_1")
TP = ("tp_0", "tp_1")
LANES = 128
SEQ_ROWS = 16
F32 = jnp.float32
BF16 = jnp.bfloat16


def lane_iota(shape):
    return lax.broadcasted_iota(jnp.int32, shape, len(shape) - 1)


def row_iota(shape):
    return lax.broadcasted_iota(jnp.int32, shape, 0)


def log_sigmoid(x):
    return jnp.minimum(x, 0.0) - jnp.log1p(jnp.exp(-jnp.abs(x)))


def key_activation(mixed):
    return (mixed * jax.nn.sigmoid(mixed) * KEY_DIM ** (-0.5)).astype(BF16)


def suffix_after(x):
    length = x.shape[-1]
    lanes = lane_iota(x.shape)

    def ahead(y, by):
        return jnp.where(lanes < length - by, pltpu.roll(y, length - by, y.ndim - 1), 0.0)

    total = ahead(x, 1)
    by = 1
    while by < length:
        total = total + ahead(total, by)
        by *= 2
    return total


def state_kernel(bias_ref, x_ref, wk_ref, wv_ref, wi_ref, wf_ref, taps_ref, extra_ref, out_ref, w_ref, spread_ref):
    s = pl.program_id(0)
    rows = x_ref.shape[1]
    width = x_ref.shape[2]
    half = lane_iota((1, LANES)) < KEY_DIM

    @pl.when(s == 0)
    def _():
        w_ref[:, :LANES] = wk_ref[...]
        pad = jnp.zeros((6, LANES), F32)
        tail = jnp.zeros((LANES - 16, LANES), F32)
        for c in range(width // LANES):
            cols = slice(c * LANES, (c + 1) * LANES)
            gates = jnp.concatenate(
                [wi_ref[:, cols].astype(F32), pad, wf_ref[:, cols].astype(F32), pad, tail], axis=0
            )
            w_ref[cols, LANES:] = gates.T.astype(BF16)
        spot = lax.broadcasted_iota(jnp.int32, spread_ref.shape, 0)
        lane = lane_iota(spread_ref.shape)
        goal = (spot // LANES) * 8 + spot % 8
        spread_ref[...] = jnp.where(goal == lane, 1.0, 0.0).astype(BF16)

    x = x_ref[0]
    key_gate = jnp.dot(x, w_ref[...], preferred_element_type=F32)
    values = jnp.dot(x, wv_ref[...], preferred_element_type=F32).astype(BF16)
    raw_bf = key_gate[:, :LANES].astype(BF16)
    raw = raw_bf.astype(F32)
    gates = key_gate[:, LANES:].T
    input_pre = gates[0:2].astype(BF16).astype(F32)
    forget_pre = gates[8:10].astype(BF16).astype(F32)
    bias = jnp.where(row_iota((2, 1)) == 0, bias_ref[0], bias_ref[1])
    log_forget = log_sigmoid(forget_pre + bias) + extra_ref[0]
    gate_log = input_pre + suffix_after(log_forget)
    peak = jnp.max(gate_log, axis=1, keepdims=True)
    seg_total = jnp.sum(log_forget, axis=1, keepdims=True)
    scale = jnp.exp(gate_log - peak)

    taps = taps_ref[...].astype(F32)
    before = pltpu.roll(raw, 1, 0)
    after = pltpu.roll(raw, rows - 1, 0)
    mixed = taps[0:1] * before + taps[1:2] * raw + taps[2:3] * after
    place = row_iota((rows, 1))
    inner = (place > 0) & (place < rows - 1)
    key_rows = jnp.where(inner, key_activation(mixed).astype(F32), 0.0)
    key_t = key_rows.T
    scaled_t = jnp.concatenate([key_t[:KEY_DIM] * scale[0:1], key_t[KEY_DIM:] * scale[1:2]], axis=0)
    memory = jnp.dot(scaled_t.astype(BF16), values, preferred_element_type=F32)
    memory = jnp.concatenate([memory[:KEY_DIM, :LANES], memory[KEY_DIM:, LANES:]], axis=0).T
    owners = LANES // 8
    base = pl.multiple_of(s * SEQ_ROWS, 8)
    out_ref[:, pl.ds(base, 8), :] = memory.reshape(owners, 8, LANES)

    high = scale.astype(BF16).astype(F32)
    middle = (scale - high).astype(BF16).astype(F32)
    low = scale - high - middle
    pieces = jnp.concatenate([high, middle, low, jnp.zeros_like(low)], axis=0).astype(BF16)
    norm = jnp.dot(pieces, key_rows.astype(BF16), preferred_element_type=F32)
    norm = jnp.where(half, norm[0:1] + norm[2:3] + norm[4:5], norm[1:2] + norm[3:4] + norm[5:6])

    ends = []
    for at in (0, rows - 1):
        for h in range(2):
            row = values[at : at + 1, h * LANES : (h + 1) * LANES].astype(F32)
            ends.append(row * scale[h : h + 1, at : at + 1])
    ends = jnp.concatenate(ends, axis=1)
    spot = lax.broadcasted_iota(jnp.int32, (owners, ends.shape[1]), 1)
    mine = (spot % LANES) // 8 == row_iota((owners, 1))
    picked = jnp.where(mine, ends, 0.0).astype(BF16)
    by_owner = jnp.dot(picked, spread_ref[...], preferred_element_type=F32)
    lane = lane_iota((1, LANES))
    last = jnp.zeros((1, LANES), F32)
    for p, at in enumerate((0, rows - 1)):
        for h in range(2):
            last = jnp.where(lane == 32 + 2 * p + h, scale[h : h + 1, at : at + 1], last)
    shared = jnp.concatenate(
        [
            raw[0:2],
            raw[rows - 2 : rows],
            norm,
            jnp.where(half, peak[0:1], peak[1:2]),
            jnp.where(half, seg_total[0:1], seg_total[1:2]),
            last,
        ],
        axis=0,
    )
    by_owner = jnp.where(row_iota((8, LANES))[None] == 7, by_owner[:, None, :], 0.0)
    out_ref[:, pl.ds(base + 8, 8), :] = shared[None] + by_owner


def prompt_states(prompt, key_weight, value_weight, input_gate_t, forget_gate_t, forget_bias, key_taps, extra_t):
    seqs, rows, width = prompt.shape
    owners = LANES // 8
    whole = lambda a: pl.BlockSpec(a.shape, lambda s: (0,) * a.ndim)
    return pl.pallas_call(
        state_kernel,
        grid=(seqs,),
        in_specs=[
            pl.BlockSpec(memory_space=pltpu.SMEM),
            pl.BlockSpec((1, rows, width), lambda s: (s, 0, 0)),
            whole(key_weight),
            whole(value_weight),
            whole(input_gate_t),
            whole(forget_gate_t),
            whole(key_taps),
            pl.BlockSpec((1, 2, rows), lambda s: (s, 0, 0)),
        ],
        out_specs=pl.BlockSpec((owners, seqs * SEQ_ROWS, LANES), lambda s: (0, 0, 0)),
        out_shape=jax.ShapeDtypeStruct((owners, seqs * SEQ_ROWS, LANES), F32),
        scratch_shapes=[pltpu.VMEM((width, 2 * LANES), BF16), pltpu.VMEM((4 * LANES, LANES), BF16)],
        compiler_params=pltpu.CompilerParams(vmem_limit_bytes=48 * 1024 * 1024),
        name="prompt_states",
    )(forget_bias, prompt, key_weight, value_weight, input_gate_t, forget_gate_t, key_taps, extra_t)


def read_kernel(
    index_ref, forget_ref, gate_ref, parts_ref, taps_ref, query_ref, key_ref, value_ref, weight_ref,
    memory_out, norm_out, peak_out, sent_out,
):
    devices = parts_ref.shape[0]
    seqs = query_ref.shape[0]
    half = lane_iota((1, LANES)) < KEY_DIM
    device = row_iota((devices, 1))
    taps = taps_ref[...].astype(F32)
    down = lambda y, by: jnp.where(device < devices - by, pltpu.roll(y, devices - by, 0), 0.0)
    reads = [jnp.zeros((8, LANES), F32), jnp.zeros((8, LANES), F32)]
    peaks = jnp.zeros((2, seqs), F32)
    for s in range(seqs):
        base = s * SEQ_ROWS
        row = lambda r: parts_ref[:, base + 8 + r, :]
        later = down(row(6), 1)
        for by in (1, 2, 4, 8):
            later = later + down(later, by)
        level = row(5) + later
        peak = jnp.max(level, axis=0, keepdims=True)
        factor = jnp.exp(level - peak)
        before = jnp.where(device > 0, pltpu.roll(row(3), 1, 0), 0.0)
        first = key_activation(taps[0:1] * before + taps[1:2] * row(0) + taps[2:3] * row(1)).astype(F32)
        last = key_activation(taps[0:1] * row(2) + taps[1:2] * row(3) + taps[2:3] * down(row(0), 1)).astype(F32)
        ends = row(7)
        contract = (((0,), (0,)), ((), ()))
        at_first, at_last = (
            lax.dot_general(ends, rows * factor, contract, precision=lax.Precision.HIGHEST, preferred_element_type=F32)
            for rows in (first, last)
        )
        edge = jnp.where(half, at_first[0:8] + at_last[16:24], at_first[8:16] + at_last[24:32])
        norm_edge = jnp.where(half, at_first[32:33] + at_last[34:35], at_first[33:34] + at_last[35:36])
        memory = edge + jnp.sum(parts_ref[:, base : base + 8, :] * factor[:, None, :], axis=0)
        norm = norm_edge + jnp.sum(row(4) * factor, axis=0, keepdims=True)
        memory_bf = memory.astype(BF16)
        memory_out[s, 0] = memory_bf[:, :KEY_DIM]
        memory_out[s, 1] = memory_bf[:, KEY_DIM:]
        own = pltpu.roll(norm, LANES - index_ref[0] * 4, 1)
        norm_out[s, 0:1, :] = own[:, 0:4].astype(BF16)
        norm_out[s, 1:2, :] = own[:, KEY_DIM : KEY_DIM + 4].astype(BF16)

        forget = log_sigmoid(jnp.where(half, forget_ref[s, 0], forget_ref[s, 1]))
        gate = jnp.where(half, gate_ref[s, 0], gate_ref[s, 1])
        new_peak = jnp.maximum(forget + peak, gate)
        old_scale = jnp.exp(forget + peak - new_peak)
        new_scale = jnp.exp(gate - new_peak)
        query = query_ref[s : s + 1]
        new_key = new_scale * key_ref[s : s + 1]
        numer = query * (old_scale * memory + new_key * value_ref[s])
        denom = query * (old_scale * norm + new_key)
        spot = lane_iota((8, LANES))
        for h in range(2):
            side = half if h == 0 else jnp.logical_not(half)
            top = jnp.sum(jnp.where(side, numer, 0.0), axis=1, keepdims=True)
            bottom = jnp.sum(jnp.where(side, denom, 0.0), axis=1, keepdims=True)
            read = top / jnp.maximum(jnp.abs(bottom), 1.0)
            reads[h] = jnp.where((spot & 3) == s, read, reads[h])
            mark = (lane_iota(peaks.shape) == s) & (row_iota(peaks.shape) == h)
            peaks = jnp.where(mark, peak[:, h * KEY_DIM : h * KEY_DIM + 1], peaks)
    peak_out[...] = peaks
    read_rows = jnp.concatenate(reads, axis=0).T[0:8].astype(BF16)
    partial = jnp.dot(read_rows, weight_ref[...], preferred_element_type=F32)
    sub = row_iota((8, LANES))
    block = lane_iota((8, LANES)) // 32
    for m in range(partial.shape[1] // (2 * LANES)):
        low = partial[:, 2 * m * LANES : (2 * m + 1) * LANES]
        high = partial[:, (2 * m + 1) * LANES : (2 * m + 2) * LANES]
        both = jnp.where(sub < 4, low, high)
        out = jnp.zeros_like(both)
        for r in range(4):
            moved = pltpu.roll(both, 32 * r, 1) if r else both
            if r:
                near = pltpu.roll(moved, 8 - r, 0)
                wrap = pltpu.roll(moved, 4 - r, 0)
                moved = jnp.where((sub & 3) + r < 4, near, wrap)
            out = jnp.where(block == (((sub & 3) + r) & 3), moved, out)
        sent_out[8 * m : 8 * m + 8, :] = out


def first_read(index, forget, gate, parts, taps, query, key, value, weight):
    seqs = query.shape[0]
    vmem = pl.BlockSpec(memory_space=pltpu.VMEM)
    smem = pl.BlockSpec(memory_space=pltpu.SMEM)
    devices_all = weight.shape[1] // 32
    return pl.pallas_call(
        read_kernel,
        in_specs=[smem, smem, smem] + [vmem] * 6,
        out_specs=[vmem] * 4,
        out_shape=[
            jax.ShapeDtypeStruct((seqs, 2, 8, KEY_DIM), BF16),
            jax.ShapeDtypeStruct((seqs, 2, 4), BF16),
            jax.ShapeDtypeStruct((2, seqs), F32),
            jax.ShapeDtypeStruct((devices_all, LANES), F32),
        ],
        compiler_params=pltpu.CompilerParams(vmem_limit_bytes=32 * 1024 * 1024),
        name="first_read",
    )(index, forget, gate, parts, taps, query, key, value, weight)


def sum_kernel(parts_ref, out_ref):
    total = jnp.sum(parts_ref[...], axis=0, keepdims=True)
    for s in range(out_ref.shape[0]):
        out_ref[s : s + 1, :] = total[:, 32 * s : 32 * s + 32].astype(BF16)


def sum_parts(parts, seqs):
    vmem = pl.BlockSpec(memory_space=pltpu.VMEM)
    return pl.pallas_call(
        sum_kernel,
        in_specs=[vmem],
        out_specs=vmem,
        out_shape=jax.ShapeDtypeStruct((seqs, 32), BF16),
        name="sum_parts",
    )(parts)


def body(
    prompt, key_weight, value_weight, input_gate_weight, forget_gate_weight, forget_bias, key_taps,
    extra_decay, new_query, new_key, new_value, new_input_gate, new_forget_gate, out_weight,
):
    seqs = prompt.shape[0]
    index = lax.axis_index(SP).reshape(1)
    parts = prompt_states(
        prompt, key_weight, value_weight, input_gate_weight.T, forget_gate_weight.T, forget_bias,
        key_taps, extra_decay.transpose(0, 2, 1),
    )
    query = new_query.astype(F32).reshape(seqs, LANES)
    key = new_key.astype(F32).reshape(seqs, LANES)
    value = jnp.repeat(new_value.astype(F32).transpose(0, 2, 1), KEY_DIM, axis=2)
    parts = lax.all_to_all(parts, SP, 0, 0, tiled=True)
    memory, norm, peak, sent = first_read(
        index, new_forget_gate, new_input_gate, parts, key_taps, query, key, value,
        out_weight.reshape(-1, out_weight.shape[2]),
    )
    got = lax.all_to_all(sent.reshape(-1, 1, LANES), SP_TP, 0, 0, tiled=True)
    read_out = sum_parts(got.reshape(-1, LANES), seqs)
    return memory.swapaxes(2, 3), norm, peak.T, read_out


def solution(mesh):
    torus = Mesh(mesh.devices.reshape(4, 4, 4, 2), ("sp_0", "sp_1", "tp_0", "tp_1"))
    in_specs = (
        P(None, SP, None), P(None, TP), P(None, TP), P(None, TP), P(None, TP), P(TP), P(None, TP),
        P(None, SP, TP), P(None, TP, None), P(None, TP, None), P(None, TP, SP), P(None, TP), P(None, TP),
        P(TP, SP, None),
    )
    out_specs = (P(None, TP, None, SP), P(None, TP, SP), P(None, TP), P(None, SP_TP))
    return jax.shard_map(body, mesh=torus, in_specs=in_specs, out_specs=out_specs, check_vma=False)
```

```python
import jax
import jax.numpy as jnp
from jax import lax
from jax.experimental import pallas as pl
from jax.experimental.pallas import tpu as pltpu
from jax.sharding import Mesh
from jax.sharding import PartitionSpec as P

KEY_DIM = 64
SP = ("sp_0", "sp_1")
SP_TP = ("sp_0", "sp_1", "tp_0", "tp_1")
TP = ("tp_0", "tp_1")
LANES = 128
COPY_ROWS = 256
AHEAD = 4
PLAN = (512, 512, 512, 512)
SEQ_ROWS = 16
ENDS_AT = 32
F32 = jnp.float32
BF16 = jnp.bfloat16


def lane_iota(shape):
    return lax.broadcasted_iota(jnp.int32, shape, len(shape) - 1)


def row_iota(shape):
    return lax.broadcasted_iota(jnp.int32, shape, 0)


def log_sigmoid(x):
    return jnp.minimum(x, 0.0) - jnp.log1p(jnp.exp(-jnp.abs(x)))


def key_activation(mixed):
    return (mixed * jax.nn.sigmoid(mixed) * KEY_DIM ** (-0.5)).astype(BF16)


def split(x):
    high = x.astype(BF16).astype(F32)
    middle = (x - high).astype(BF16).astype(F32)
    return [high, middle, x - high - middle]


def suffix_after(x):
    length = x.shape[-1]
    lanes = lane_iota(x.shape)

    def ahead(y, by):
        return jnp.where(lanes < length - by, pltpu.roll(y, length - by, y.ndim - 1), 0.0)

    total = ahead(x, 1)
    by = 1
    while by < length:
        total = total + ahead(total, by)
        by *= 2
    return total


def state_kernel(
    x_hbm, wk_hbm, wv_hbm, wi_hbm, wf_hbm, bias_hbm, taps_hbm, extra_hbm, out_ref,
    x_ref, w_ref, wi_ref, wf_ref, bias_ref, taps_ref, extra_ref, spread_ref, raw_ref, gate_ref, value_ref,
    x_sem, w_sem, small_sem,
):
    seqs, _, rows = extra_ref.shape
    total_rows, width = x_ref.shape
    owners = LANES // 8
    half = lane_iota((1, LANES)) < KEY_DIM

    small = [
        pltpu.make_async_copy(src, dst, small_sem.at[i])
        for i, (src, dst) in enumerate(
            [(wi_hbm, wi_ref), (wf_hbm, wf_ref), (bias_hbm, bias_ref), (taps_hbm, taps_ref), (extra_hbm, extra_ref)]
        )
    ]
    weights = [
        pltpu.make_async_copy(wk_hbm, w_ref.at[:, 0:LANES], w_sem.at[0]),
        pltpu.make_async_copy(wv_hbm, w_ref.at[:, 2 * LANES : 4 * LANES], w_sem.at[1]),
    ]
    blocks = [
        pltpu.make_async_copy(x_hbm.at[pl.ds(at, COPY_ROWS)], x_ref.at[pl.ds(at, COPY_ROWS)], x_sem.at[at // COPY_ROWS])
        for at in range(0, total_rows, COPY_ROWS)
    ]
    for copy in small + weights:
        copy.start()
    for copy in blocks[:AHEAD]:
        copy.start()
    for copy in small:
        copy.wait()

    pad = jnp.zeros((6, LANES), F32)
    tail = jnp.zeros((LANES - 16, LANES), F32)
    for c in range(width // LANES):
        cols = slice(c * LANES, (c + 1) * LANES)
        gates = jnp.concatenate([wi_ref[:, cols].astype(F32), pad, wf_ref[:, cols].astype(F32), pad, tail], axis=0)
        w_ref[cols, LANES : 2 * LANES] = gates.T.astype(BF16)
    spot = lax.broadcasted_iota(jnp.int32, spread_ref.shape, 0)
    goal = (spot // LANES) * 8 + spot % 8
    spread_ref[...] = jnp.where(goal == lane_iota(spread_ref.shape), 1.0, 0.0).astype(BF16)
    taps = taps_ref[...].astype(F32)
    bias = jnp.where(row_iota((2, 1)) == 0, bias_ref[:, 0:1], bias_ref[:, 1:2])
    for copy in weights:
        copy.wait()

    def project(start, count):
        at = slice(start, start + count)
        key_gate = jnp.dot(x_ref[at], w_ref[:, : 2 * LANES], preferred_element_type=F32)
        value = jnp.dot(x_ref[at], w_ref[:, 2 * LANES :], preferred_element_type=F32)
        raw_ref[at] = key_gate[:, :LANES].astype(BF16)
        gate_ref[at] = key_gate[:, LANES:]
        value_ref[at] = value.astype(BF16)

    def finish(s):
        own = slice(s * rows, (s + 1) * rows)
        values = value_ref[own]
        raw = raw_ref[own].astype(F32)
        gates = gate_ref[own].T
        input_pre = gates[0:2].astype(BF16).astype(F32)
        forget_pre = gates[8:10].astype(BF16).astype(F32)
        log_forget = log_sigmoid(forget_pre + bias) + extra_ref[s]
        gate_log = input_pre + suffix_after(log_forget)
        peak = jnp.max(gate_log, axis=1, keepdims=True)
        seg_total = jnp.sum(log_forget, axis=1, keepdims=True)
        scale = jnp.exp(gate_log - peak)

        before = pltpu.roll(raw, 1, 0)
        after = pltpu.roll(raw, rows - 1, 0)
        mixed = taps[0:1] * before + taps[1:2] * raw + taps[2:3] * after
        place = row_iota((rows, 1))
        inner = (place > 0) & (place < rows - 1)
        key_rows = jnp.where(inner, key_activation(mixed).astype(F32), 0.0)
        key_t = key_rows.T
        scaled_t = jnp.concatenate([key_t[:KEY_DIM] * scale[0:1], key_t[KEY_DIM:] * scale[1:2]], axis=0)
        memory = jnp.dot(scaled_t.astype(BF16), values, preferred_element_type=F32)
        memory = jnp.concatenate([memory[:KEY_DIM, :LANES], memory[KEY_DIM:, LANES:]], axis=0).T

        scale_parts = split(scale)
        pieces = jnp.concatenate(scale_parts + [jnp.zeros_like(scale)], axis=0).astype(BF16)
        norm = jnp.dot(pieces, key_rows.astype(BF16), preferred_element_type=F32)
        norm = jnp.where(half, norm[0:1] + norm[2:3] + norm[4:5], norm[1:2] + norm[3:4] + norm[5:6])

        ends = []
        for at in (0, rows - 1):
            for h in range(2):
                row = values[at : at + 1, h * LANES : (h + 1) * LANES].astype(F32)
                ends.append(row * scale[h : h + 1, at : at + 1])
        ends = jnp.concatenate(ends, axis=1)
        spot = lax.broadcasted_iota(jnp.int32, (owners, ends.shape[1]), 1)
        mine = (spot % LANES) // 8 == row_iota((owners, 1))
        picked = jnp.where(mine, ends, 0.0).astype(BF16)
        by_owner = jnp.dot(picked, spread_ref[...], preferred_element_type=F32)
        lane = lane_iota((1, LANES))
        ends_row = jnp.zeros((1, LANES), F32)
        stats_row = jnp.zeros((1, LANES), F32)
        for i, part in enumerate(scale_parts[:2]):
            for p, at in enumerate((0, rows - 1)):
                for h in range(2):
                    ends_row = jnp.where(lane == ENDS_AT + 4 * i + 2 * p + h, part[h : h + 1, at : at + 1], ends_row)
        for i, part in enumerate(split(peak) + split(seg_total)):
            for h in range(2):
                stats_row = jnp.where(lane == 2 * i + h, part[h : h + 1], stats_row)
        shared = jnp.concatenate([raw[0:2], raw[rows - 2 : rows]] + split(norm)[:2] + [ends_row, stats_row], axis=0)
        by_owner = jnp.where(row_iota((8, LANES))[None] == 6, by_owner[:, None, :], 0.0)
        block = jnp.concatenate([memory.reshape(owners, 8, LANES), shared[None] + by_owner], axis=1)
        out_ref[:, s * SEQ_ROWS : (s + 1) * SEQ_ROWS, :] = block.astype(BF16)

    done = 0
    finished = 0
    for count in PLAN:
        for i in range(done // COPY_ROWS, (done + count) // COPY_ROWS):
            blocks[i].wait()
            if i + AHEAD < len(blocks):
                blocks[i + AHEAD].start()
        project(done, count)
        ready = done // rows
        for s in range(finished, ready):
            finish(s)
        finished = ready
        done += count
    for s in range(finished, seqs):
        finish(s)


def prompt_states(prompt, key_weight, value_weight, input_gate_t, forget_gate_t, forget_bias, key_taps, extra_t):
    seqs, rows, width = prompt.shape
    owners = LANES // 8
    return pl.pallas_call(
        state_kernel,
        in_specs=[pl.BlockSpec(memory_space=pltpu.HBM)] * 8,
        out_specs=pl.BlockSpec(memory_space=pltpu.VMEM),
        out_shape=jax.ShapeDtypeStruct((owners, seqs * SEQ_ROWS, LANES), BF16),
        scratch_shapes=[
            pltpu.VMEM((seqs * rows, width), BF16),
            pltpu.VMEM((width, 4 * LANES), BF16),
            pltpu.VMEM(input_gate_t.shape, BF16),
            pltpu.VMEM(forget_gate_t.shape, BF16),
            pltpu.VMEM(forget_bias.shape, F32),
            pltpu.VMEM(key_taps.shape, BF16),
            pltpu.VMEM(extra_t.shape, F32),
            pltpu.VMEM((4 * LANES, LANES), BF16),
            pltpu.VMEM((seqs * rows, LANES), BF16),
            pltpu.VMEM((seqs * rows, LANES), F32),
            pltpu.VMEM((seqs * rows, 2 * LANES), BF16),
            pltpu.SemaphoreType.DMA((seqs * rows // COPY_ROWS,)),
            pltpu.SemaphoreType.DMA((2,)),
            pltpu.SemaphoreType.DMA((5,)),
        ],
        compiler_params=pltpu.CompilerParams(vmem_limit_bytes=60 * 1024 * 1024),
        name="prompt_states",
    )(prompt.reshape(seqs * rows, width), key_weight, value_weight, input_gate_t, forget_gate_t, forget_bias, key_taps, extra_t)


def paired(ref, s):
    rows = ref[s].astype(F32)
    return jnp.concatenate([rows[0:1], rows[1:2]], axis=1)


def read_kernel(
    index_ref, forget_ref, gate_ref, parts_ref, taps_ref, query_ref, key_ref, value_ref, weight_ref,
    memory_out, norm_out, peak_out, sent_out,
):
    devices = parts_ref.shape[0]
    seqs = query_ref.shape[0]
    half = lane_iota((1, LANES)) < KEY_DIM
    heads = jnp.where(half == (row_iota((2, LANES)) == 0), 1.0, 0.0).astype(BF16)
    device = row_iota((devices, 1))
    taps = taps_ref[...].astype(F32)
    contract = (((0,), (0,)), ((), ()))
    down = lambda y, by: jnp.where(device < devices - by, pltpu.roll(y, devices - by, 0), 0.0)
    reads = [jnp.zeros((8, LANES), F32), jnp.zeros((8, LANES), F32)]
    peaks = jnp.zeros((2, seqs), F32)
    for s in range(seqs):
        parts = parts_ref[:, s * SEQ_ROWS : (s + 1) * SEQ_ROWS, :].astype(F32)
        row = lambda r: parts[:, 8 + r, :]
        stats = row(7)

        def joined(first):
            ones = [stats[:, first + 2 * i : first + 2 * i + 1] for i in range(3)]
            twos = [stats[:, first + 2 * i + 1 : first + 2 * i + 2] for i in range(3)]
            return jnp.where(half, ones[0] + ones[1] + ones[2], twos[0] + twos[1] + twos[2])

        later = down(joined(6), 1)
        for by in (1, 2, 4, 8):
            later = later + down(later, by)
        level = joined(0) + later
        peak = jnp.max(level, axis=0, keepdims=True)
        factor = jnp.exp(level - peak)
        before = jnp.where(device > 0, pltpu.roll(row(3), 1, 0), 0.0)
        first = key_activation(taps[0:1] * before + taps[1:2] * row(0) + taps[2:3] * row(1)).astype(F32)
        last = key_activation(taps[0:1] * row(2) + taps[1:2] * row(3) + taps[2:3] * down(row(0), 1)).astype(F32)
        ends = row(6)
        at_first, at_last = (
            lax.dot_general(ends, rows * factor, contract, precision=lax.Precision.HIGHEST, preferred_element_type=F32)
            for rows in (first, last)
        )
        edge = jnp.where(half, at_first[0:8] + at_last[16:24], at_first[8:16] + at_last[24:32])
        scaled = at_first[32:33] + at_first[36:37] + at_last[34:35] + at_last[38:39]
        scaled_two = at_first[33:34] + at_first[37:38] + at_last[35:36] + at_last[39:40]
        norm_edge = jnp.where(half, scaled, scaled_two)
        memory = edge + jnp.sum(parts[:, 0:8, :] * factor[:, None, :], axis=0)
        norm = norm_edge + jnp.sum((row(4) + row(5)) * factor, axis=0, keepdims=True)
        memory_bf = memory.astype(BF16)
        memory_out[s, 0] = memory_bf[:, :KEY_DIM]
        memory_out[s, 1] = memory_bf[:, KEY_DIM:]
        own = pltpu.roll(norm, LANES - index_ref[0] * 4, 1)
        norm_out[s, 0:1, :] = own[:, 0:4].astype(BF16)
        norm_out[s, 1:2, :] = own[:, KEY_DIM : KEY_DIM + 4].astype(BF16)

        forget = log_sigmoid(jnp.where(half, forget_ref[0, s], forget_ref[1, s]))
        gate = jnp.where(half, gate_ref[0, s], gate_ref[1, s])
        new_peak = jnp.maximum(forget + peak, gate)
        old_scale = jnp.exp(forget + peak - new_peak)
        new_scale = jnp.exp(gate - new_peak)
        query = paired(query_ref, s)
        new_key = new_scale * paired(key_ref, s)
        new_value = lax.dot_general(value_ref[s], heads, contract, preferred_element_type=F32)
        numer = query * (old_scale * memory + new_key * new_value)
        denom = query * (old_scale * norm + new_key)
        spot = lane_iota((8, LANES))
        for h in range(2):
            side = half if h == 0 else jnp.logical_not(half)
            top = jnp.sum(jnp.where(side, numer, 0.0), axis=1, keepdims=True)
            bottom = jnp.sum(jnp.where(side, denom, 0.0), axis=1, keepdims=True)
            read = top / jnp.maximum(jnp.abs(bottom), 1.0)
            reads[h] = jnp.where((spot & 3) == s, read, reads[h])
            mark = (lane_iota(peaks.shape) == s) & (row_iota(peaks.shape) == h)
            peaks = jnp.where(mark, peak[:, h * KEY_DIM : h * KEY_DIM + 1], peaks)
    peak_out[...] = peaks
    read_rows = jnp.concatenate(reads, axis=0).T[0:8].astype(BF16)
    partial = jnp.dot(read_rows, weight_ref[...], preferred_element_type=F32)
    sub = row_iota((8, LANES))
    block = lane_iota((8, LANES)) // 32
    for m in range(partial.shape[1] // (2 * LANES)):
        low = partial[:, 2 * m * LANES : (2 * m + 1) * LANES]
        high = partial[:, (2 * m + 1) * LANES : (2 * m + 2) * LANES]
        both = jnp.where(sub < 4, low, high)
        out = jnp.zeros_like(both)
        for r in range(4):
            moved = pltpu.roll(both, 32 * r, 1) if r else both
            if r:
                near = pltpu.roll(moved, 8 - r, 0)
                wrap = pltpu.roll(moved, 4 - r, 0)
                moved = jnp.where((sub & 3) + r < 4, near, wrap)
            out = jnp.where(block == (((sub & 3) + r) & 3), moved, out)
        sent_out[8 * m : 8 * m + 8, :] = out


def first_read(index, forget, gate, parts, taps, query, key, value, weight):
    seqs = query.shape[0]
    vmem = pl.BlockSpec(memory_space=pltpu.VMEM)
    smem = pl.BlockSpec(memory_space=pltpu.SMEM)
    devices_all = weight.shape[1] // 32
    return pl.pallas_call(
        read_kernel,
        in_specs=[smem, smem, smem] + [vmem] * 6,
        out_specs=[vmem] * 4,
        out_shape=[
            jax.ShapeDtypeStruct((seqs, 2, 8, KEY_DIM), BF16),
            jax.ShapeDtypeStruct((seqs, 2, 4), BF16),
            jax.ShapeDtypeStruct((2, seqs), F32),
            jax.ShapeDtypeStruct((devices_all, LANES), F32),
        ],
        compiler_params=pltpu.CompilerParams(vmem_limit_bytes=32 * 1024 * 1024),
        name="first_read",
    )(index, forget, gate, parts, taps, query, key, value, weight)


def sum_kernel(parts_ref, out_ref):
    total = jnp.sum(parts_ref[...], axis=0, keepdims=True)
    for s in range(out_ref.shape[0]):
        out_ref[s : s + 1, :] = total[:, 32 * s : 32 * s + 32].astype(BF16)


def sum_parts(parts, seqs):
    vmem = pl.BlockSpec(memory_space=pltpu.VMEM)
    return pl.pallas_call(
        sum_kernel,
        in_specs=[vmem],
        out_specs=vmem,
        out_shape=jax.ShapeDtypeStruct((seqs, 32), BF16),
        name="sum_parts",
    )(parts)


def body(
    prompt, key_weight, value_weight, input_gate_weight, forget_gate_weight, forget_bias, key_taps,
    extra_decay, new_query, new_key, new_value, new_input_gate, new_forget_gate, out_weight,
):
    seqs = prompt.shape[0]
    index = lax.axis_index(SP).reshape(1)
    parts = prompt_states(
        prompt, key_weight, value_weight, input_gate_weight.T, forget_gate_weight.T, forget_bias.reshape(1, -1),
        key_taps, extra_decay.transpose(0, 2, 1),
    )
    parts = lax.all_to_all(parts, SP, 0, 0, tiled=True)
    memory, norm, peak, sent = first_read(
        index, new_forget_gate.T, new_input_gate.T, parts, key_taps, new_query, new_key, new_value,
        out_weight.reshape(-1, out_weight.shape[2]),
    )
    got = lax.all_to_all(sent.reshape(-1, 1, LANES), SP_TP, 0, 0, tiled=True)
    read_out = sum_parts(got.reshape(-1, LANES), seqs)
    return memory.swapaxes(2, 3), norm, peak.T, read_out


def solution(mesh):
    torus = Mesh(mesh.devices.reshape(4, 4, 4, 2), ("sp_0", "sp_1", "tp_0", "tp_1"))
    in_specs = (
        P(None, SP, None), P(None, TP), P(None, TP), P(None, TP), P(None, TP), P(TP), P(None, TP),
        P(None, SP, TP), P(None, TP, None), P(None, TP, None), P(None, TP, SP), P(None, TP), P(None, TP),
        P(TP, SP, None),
    )
    out_specs = (P(None, TP, None, SP), P(None, TP, SP), P(None, TP), P(None, SP_TP))
    return jax.shard_map(body, mesh=torus, in_specs=in_specs, out_specs=out_specs, check_vma=False)
```

```python
import jax
import jax.numpy as jnp
from jax import lax
from jax.experimental import pallas as pl
from jax.experimental.pallas import tpu as pltpu
from jax.sharding import Mesh
from jax.sharding import PartitionSpec as P

KEY_DIM = 64
SP = ("sp_0", "sp_1")
SP_TP = ("sp_0", "sp_1", "tp_0", "tp_1")
TP = ("tp_0", "tp_1")
LANES = 128
COPY_ROWS = 256
FIRST = 1
AHEAD = 2
PLAN = (256, 512, 512, 512, 256)
SEQ_ROWS = 16
ENDS_AT = 32
F32 = jnp.float32
BF16 = jnp.bfloat16


def lane_iota(shape):
    return lax.broadcasted_iota(jnp.int32, shape, len(shape) - 1)


def row_iota(shape):
    return lax.broadcasted_iota(jnp.int32, shape, 0)


def log_sigmoid(x):
    return jnp.minimum(x, 0.0) - jnp.log1p(jnp.exp(-jnp.abs(x)))


def key_activation(mixed):
    return (mixed * jax.nn.sigmoid(mixed) * KEY_DIM ** (-0.5)).astype(BF16)


def split(x):
    high = x.astype(BF16).astype(F32)
    middle = (x - high).astype(BF16).astype(F32)
    return [high, middle, x - high - middle]


def suffix_after(x):
    length = x.shape[-1]
    lanes = lane_iota(x.shape)

    def ahead(y, by):
        return jnp.where(lanes < length - by, pltpu.roll(y, length - by, y.ndim - 1), 0.0)

    total = ahead(x, 1)
    by = 1
    while by < length:
        total = total + ahead(total, by)
        by *= 2
    return total


def state_kernel(
    x_hbm, wk_hbm, wv_hbm, wi_hbm, wf_hbm, bias_hbm, taps_hbm, extra_hbm, out_ref,
    x_ref, w_ref, wi_ref, wf_ref, bias_ref, taps_ref, extra_ref, spread_ref, raw_ref, gate_ref, value_ref,
    x_sem, w_sem, small_sem,
):
    seqs, _, rows = extra_ref.shape
    total_rows, width = x_ref.shape
    owners = LANES // 8
    half = lane_iota((1, LANES)) < KEY_DIM

    small = [
        pltpu.make_async_copy(src, dst, small_sem.at[i])
        for i, (src, dst) in enumerate(
            [(wi_hbm, wi_ref), (wf_hbm, wf_ref), (bias_hbm, bias_ref), (taps_hbm, taps_ref), (extra_hbm, extra_ref)]
        )
    ]
    weights = [
        pltpu.make_async_copy(wk_hbm, w_ref.at[:, 0:LANES], w_sem.at[0]),
        pltpu.make_async_copy(wv_hbm, w_ref.at[:, 2 * LANES : 4 * LANES], w_sem.at[1]),
    ]
    blocks = [
        pltpu.make_async_copy(x_hbm.at[pl.ds(at, COPY_ROWS)], x_ref.at[pl.ds(at, COPY_ROWS)], x_sem.at[at // COPY_ROWS])
        for at in range(0, total_rows, COPY_ROWS)
    ]
    for copy in small + weights[:1] + blocks[:FIRST] + weights[1:] + blocks[FIRST:AHEAD]:
        copy.start()
    for copy in small:
        copy.wait()

    pad = jnp.zeros((6, LANES), F32)
    tail = jnp.zeros((LANES - 16, LANES), F32)
    for c in range(width // LANES):
        cols = slice(c * LANES, (c + 1) * LANES)
        gates = jnp.concatenate([wi_ref[:, cols].astype(F32), pad, wf_ref[:, cols].astype(F32), pad, tail], axis=0)
        w_ref[cols, LANES : 2 * LANES] = gates.T.astype(BF16)
    spot = lax.broadcasted_iota(jnp.int32, spread_ref.shape, 0)
    goal = (spot // LANES) * 8 + spot % 8
    spread_ref[...] = jnp.where(goal == lane_iota(spread_ref.shape), 1.0, 0.0).astype(BF16)
    taps = taps_ref[...].astype(F32)
    bias = jnp.where(row_iota((2, 1)) == 0, bias_ref[:, 0:1], bias_ref[:, 1:2])
    weights[0].wait()

    def project(start, count):
        at = slice(start, start + count)
        key_gate = jnp.dot(x_ref[at], w_ref[:, : 2 * LANES], preferred_element_type=F32)
        if start == 0:
            weights[1].wait()
        value = jnp.dot(x_ref[at], w_ref[:, 2 * LANES :], preferred_element_type=F32)
        raw_ref[at] = key_gate[:, :LANES].astype(BF16)
        gate_ref[at] = key_gate[:, LANES:]
        value_ref[at] = value.astype(BF16)

    def finish(s):
        own = slice(s * rows, (s + 1) * rows)
        values = value_ref[own]
        raw = raw_ref[own].astype(F32)
        gates = gate_ref[own].T
        input_pre = gates[0:2].astype(BF16).astype(F32)
        forget_pre = gates[8:10].astype(BF16).astype(F32)
        log_forget = log_sigmoid(forget_pre + bias) + extra_ref[s]
        gate_log = input_pre + suffix_after(log_forget)
        peak = jnp.max(gate_log, axis=1, keepdims=True)
        seg_total = jnp.sum(log_forget, axis=1, keepdims=True)
        scale = jnp.exp(gate_log - peak)

        before = pltpu.roll(raw, 1, 0)
        after = pltpu.roll(raw, rows - 1, 0)
        mixed = taps[0:1] * before + taps[1:2] * raw + taps[2:3] * after
        place = row_iota((rows, 1))
        inner = (place > 0) & (place < rows - 1)
        key_rows = jnp.where(inner, key_activation(mixed).astype(F32), 0.0)
        key_t = key_rows.T
        scaled_t = jnp.concatenate([key_t[:KEY_DIM] * scale[0:1], key_t[KEY_DIM:] * scale[1:2]], axis=0)
        memory = jnp.dot(scaled_t.astype(BF16), values, preferred_element_type=F32)
        memory = jnp.concatenate([memory[:KEY_DIM, :LANES], memory[KEY_DIM:, LANES:]], axis=0).T

        scale_parts = split(scale)
        pieces = jnp.concatenate(scale_parts + [jnp.zeros_like(scale)], axis=0).astype(BF16)
        norm = jnp.dot(pieces, key_rows.astype(BF16), preferred_element_type=F32)
        norm = jnp.where(half, norm[0:1] + norm[2:3] + norm[4:5], norm[1:2] + norm[3:4] + norm[5:6])

        ends = []
        for at in (0, rows - 1):
            for h in range(2):
                row = values[at : at + 1, h * LANES : (h + 1) * LANES].astype(F32)
                ends.append(row * scale[h : h + 1, at : at + 1])
        ends = jnp.concatenate(ends, axis=1)
        spot = lax.broadcasted_iota(jnp.int32, (owners, ends.shape[1]), 1)
        mine = (spot % LANES) // 8 == row_iota((owners, 1))
        picked = jnp.where(mine, ends, 0.0).astype(BF16)
        by_owner = jnp.dot(picked, spread_ref[...], preferred_element_type=F32)
        lane = lane_iota((1, LANES))
        ends_row = jnp.zeros((1, LANES), F32)
        stats_row = jnp.zeros((1, LANES), F32)
        for i, part in enumerate(scale_parts[:2]):
            for p, at in enumerate((0, rows - 1)):
                for h in range(2):
                    ends_row = jnp.where(lane == ENDS_AT + 4 * i + 2 * p + h, part[h : h + 1, at : at + 1], ends_row)
        for i, part in enumerate(split(peak) + split(seg_total)):
            for h in range(2):
                stats_row = jnp.where(lane == 2 * i + h, part[h : h + 1], stats_row)
        shared = jnp.concatenate([raw[0:2], raw[rows - 2 : rows]] + split(norm)[:2] + [ends_row, stats_row], axis=0)
        by_owner = jnp.where(row_iota((8, LANES))[None] == 6, by_owner[:, None, :], 0.0)
        block = jnp.concatenate([memory.reshape(owners, 8, LANES), shared[None] + by_owner], axis=1)
        out_ref[:, s * SEQ_ROWS : (s + 1) * SEQ_ROWS, :] = block.astype(BF16)

    done = 0
    finished = 0
    for count in PLAN:
        for i in range(done // COPY_ROWS, (done + count) // COPY_ROWS):
            blocks[i].wait()
            if i + AHEAD < len(blocks):
                blocks[i + AHEAD].start()
        project(done, count)
        ready = done // rows
        for s in range(finished, ready):
            finish(s)
        finished = ready
        done += count
    for s in range(finished, seqs):
        finish(s)


def prompt_states(prompt, key_weight, value_weight, input_gate_t, forget_gate_t, forget_bias, key_taps, extra_t):
    seqs, rows, width = prompt.shape
    owners = LANES // 8
    return pl.pallas_call(
        state_kernel,
        in_specs=[pl.BlockSpec(memory_space=pltpu.HBM)] * 8,
        out_specs=pl.BlockSpec(memory_space=pltpu.VMEM),
        out_shape=pltpu.VMEM((owners, seqs * SEQ_ROWS, LANES), BF16),
        scratch_shapes=[
            pltpu.VMEM((seqs * rows, width), BF16),
            pltpu.VMEM((width, 4 * LANES), BF16),
            pltpu.VMEM(input_gate_t.shape, BF16),
            pltpu.VMEM(forget_gate_t.shape, BF16),
            pltpu.VMEM(forget_bias.shape, F32),
            pltpu.VMEM(key_taps.shape, BF16),
            pltpu.VMEM(extra_t.shape, F32),
            pltpu.VMEM((4 * LANES, LANES), BF16),
            pltpu.VMEM((seqs * rows, LANES), BF16),
            pltpu.VMEM((seqs * rows, LANES), F32),
            pltpu.VMEM((seqs * rows, 2 * LANES), BF16),
            pltpu.SemaphoreType.DMA((seqs * rows // COPY_ROWS,)),
            pltpu.SemaphoreType.DMA((2,)),
            pltpu.SemaphoreType.DMA((5,)),
        ],
        compiler_params=pltpu.CompilerParams(vmem_limit_bytes=60 * 1024 * 1024),
        name="prompt_states",
    )(prompt.reshape(seqs * rows, width), key_weight, value_weight, input_gate_t, forget_gate_t, forget_bias, key_taps, extra_t)


def paired(ref, s):
    rows = ref[s].astype(F32)
    return jnp.concatenate([rows[0:1], rows[1:2]], axis=1)


def read_kernel(
    index_ref, forget_ref, gate_ref, parts_ref, taps_ref, query_ref, key_ref, value_ref, weight_ref,
    memory_out, norm_out, peak_out, sent_out,
):
    devices = parts_ref.shape[0]
    seqs = query_ref.shape[0]
    half = lane_iota((1, LANES)) < KEY_DIM
    heads = jnp.where(half == (row_iota((2, LANES)) == 0), 1.0, 0.0).astype(BF16)
    device = row_iota((devices, 1))
    taps = taps_ref[...].astype(F32)
    contract = (((0,), (0,)), ((), ()))
    down = lambda y, by: jnp.where(device < devices - by, pltpu.roll(y, devices - by, 0), 0.0)
    reads = [jnp.zeros((8, LANES), F32), jnp.zeros((8, LANES), F32)]
    peaks = jnp.zeros((2, seqs), F32)
    for s in range(seqs):
        parts = parts_ref[:, s * SEQ_ROWS : (s + 1) * SEQ_ROWS, :].astype(F32)
        row = lambda r: parts[:, 8 + r, :]
        stats = row(7)

        def joined(first):
            ones = [stats[:, first + 2 * i : first + 2 * i + 1] for i in range(3)]
            twos = [stats[:, first + 2 * i + 1 : first + 2 * i + 2] for i in range(3)]
            return jnp.where(half, ones[0] + ones[1] + ones[2], twos[0] + twos[1] + twos[2])

        later = down(joined(6), 1)
        for by in (1, 2, 4, 8):
            later = later + down(later, by)
        level = joined(0) + later
        peak = jnp.max(level, axis=0, keepdims=True)
        factor = jnp.exp(level - peak)
        before = jnp.where(device > 0, pltpu.roll(row(3), 1, 0), 0.0)
        first = key_activation(taps[0:1] * before + taps[1:2] * row(0) + taps[2:3] * row(1)).astype(F32)
        last = key_activation(taps[0:1] * row(2) + taps[1:2] * row(3) + taps[2:3] * down(row(0), 1)).astype(F32)
        ends = row(6)
        at_first, at_last = (
            lax.dot_general(ends, rows * factor, contract, precision=lax.Precision.HIGHEST, preferred_element_type=F32)
            for rows in (first, last)
        )
        edge = jnp.where(half, at_first[0:8] + at_last[16:24], at_first[8:16] + at_last[24:32])
        scaled = at_first[32:33] + at_first[36:37] + at_last[34:35] + at_last[38:39]
        scaled_two = at_first[33:34] + at_first[37:38] + at_last[35:36] + at_last[39:40]
        norm_edge = jnp.where(half, scaled, scaled_two)
        memory = edge + jnp.sum(parts[:, 0:8, :] * factor[:, None, :], axis=0)
        norm = norm_edge + jnp.sum((row(4) + row(5)) * factor, axis=0, keepdims=True)
        memory_bf = memory.astype(BF16)
        memory_out[s, 0] = memory_bf[:, :KEY_DIM]
        memory_out[s, 1] = memory_bf[:, KEY_DIM:]
        own = pltpu.roll(norm, LANES - index_ref[0] * 4, 1)
        norm_out[s, 0:1, :] = own[:, 0:4].astype(BF16)
        norm_out[s, 1:2, :] = own[:, KEY_DIM : KEY_DIM + 4].astype(BF16)

        forget = log_sigmoid(jnp.where(half, forget_ref[0, s], forget_ref[1, s]))
        gate = jnp.where(half, gate_ref[0, s], gate_ref[1, s])
        new_peak = jnp.maximum(forget + peak, gate)
        old_scale = jnp.exp(forget + peak - new_peak)
        new_scale = jnp.exp(gate - new_peak)
        query = paired(query_ref, s)
        new_key = new_scale * paired(key_ref, s)
        new_value = lax.dot_general(value_ref[s], heads, contract, preferred_element_type=F32)
        numer = query * (old_scale * memory + new_key * new_value)
        denom = query * (old_scale * norm + new_key)
        spot = lane_iota((8, LANES))
        for h in range(2):
            side = half if h == 0 else jnp.logical_not(half)
            top = jnp.sum(jnp.where(side, numer, 0.0), axis=1, keepdims=True)
            bottom = jnp.sum(jnp.where(side, denom, 0.0), axis=1, keepdims=True)
            read = top / jnp.maximum(jnp.abs(bottom), 1.0)
            reads[h] = jnp.where((spot & 3) == s, read, reads[h])
            mark = (lane_iota(peaks.shape) == s) & (row_iota(peaks.shape) == h)
            peaks = jnp.where(mark, peak[:, h * KEY_DIM : h * KEY_DIM + 1], peaks)
    peak_out[...] = peaks
    read_rows = jnp.concatenate(reads, axis=0).T[0:8].astype(BF16)
    partial = jnp.dot(read_rows, weight_ref[...], preferred_element_type=F32)
    sub = row_iota((8, LANES))
    block = lane_iota((8, LANES)) // 32
    for m in range(partial.shape[1] // (2 * LANES)):
        low = partial[:, 2 * m * LANES : (2 * m + 1) * LANES]
        high = partial[:, (2 * m + 1) * LANES : (2 * m + 2) * LANES]
        both = jnp.where(sub < 4, low, high)
        out = jnp.zeros_like(both)
        for r in range(4):
            moved = pltpu.roll(both, 32 * r, 1) if r else both
            if r:
                near = pltpu.roll(moved, 8 - r, 0)
                wrap = pltpu.roll(moved, 4 - r, 0)
                moved = jnp.where((sub & 3) + r < 4, near, wrap)
            out = jnp.where(block == (((sub & 3) + r) & 3), moved, out)
        sent_out[8 * m : 8 * m + 8, :] = out


def first_read(index, forget, gate, parts, taps, query, key, value, weight):
    seqs = query.shape[0]
    vmem = pl.BlockSpec(memory_space=pltpu.VMEM)
    smem = pl.BlockSpec(memory_space=pltpu.SMEM)
    devices_all = weight.shape[1] // 32
    return pl.pallas_call(
        read_kernel,
        in_specs=[smem, smem, smem] + [vmem] * 6,
        out_specs=[vmem] * 4,
        out_shape=[
            jax.ShapeDtypeStruct((seqs, 2, 8, KEY_DIM), BF16),
            jax.ShapeDtypeStruct((seqs, 2, 4), BF16),
            jax.ShapeDtypeStruct((2, seqs), F32),
            jax.ShapeDtypeStruct((devices_all, LANES), F32),
        ],
        compiler_params=pltpu.CompilerParams(vmem_limit_bytes=32 * 1024 * 1024),
        name="first_read",
    )(index, forget, gate, parts, taps, query, key, value, weight)


def sum_kernel(parts_ref, out_ref):
    total = jnp.sum(parts_ref[...], axis=0, keepdims=True)
    for s in range(out_ref.shape[0]):
        out_ref[s : s + 1, :] = total[:, 32 * s : 32 * s + 32].astype(BF16)


def sum_parts(parts, seqs):
    vmem = pl.BlockSpec(memory_space=pltpu.VMEM)
    return pl.pallas_call(
        sum_kernel,
        in_specs=[vmem],
        out_specs=vmem,
        out_shape=jax.ShapeDtypeStruct((seqs, 32), BF16),
        compiler_params=pltpu.CompilerParams(vmem_limit_bytes=1024 * 1024),
        name="sum_parts",
    )(parts)


def body(
    prompt, key_weight, value_weight, input_gate_weight, forget_gate_weight, forget_bias, key_taps,
    extra_decay, new_query, new_key, new_value, new_input_gate, new_forget_gate, out_weight,
):
    seqs = prompt.shape[0]
    index = lax.axis_index(SP).reshape(1)
    parts = prompt_states(
        prompt, key_weight, value_weight, input_gate_weight.T, forget_gate_weight.T, forget_bias.reshape(1, -1),
        key_taps, extra_decay.transpose(0, 2, 1),
    )
    parts, index = lax.optimization_barrier((parts, index))
    parts = lax.all_to_all(parts, SP, 0, 0, tiled=True)
    memory, norm, peak, sent = first_read(
        index, new_forget_gate.T, new_input_gate.T, parts, key_taps, new_query, new_key, new_value,
        out_weight.reshape(-1, out_weight.shape[2]),
    )
    got = lax.all_to_all(sent.reshape(-1, 1, LANES), SP_TP, 0, 0, tiled=True)
    read_out = sum_parts(got.reshape(-1, LANES), seqs)
    return memory.swapaxes(2, 3), norm, peak.T, read_out


def solution(mesh):
    torus = Mesh(mesh.devices.reshape(4, 4, 4, 2), ("sp_0", "sp_1", "tp_0", "tp_1"))
    in_specs = (
        P(None, SP, None), P(None, TP), P(None, TP), P(None, TP), P(None, TP), P(TP), P(None, TP),
        P(None, SP, TP), P(None, TP, None), P(None, TP, None), P(None, TP, SP), P(None, TP), P(None, TP),
        P(TP, SP, None),
    )
    out_specs = (P(None, TP, None, SP), P(None, TP, SP), P(None, TP), P(None, SP_TP))
    return jax.shard_map(body, mesh=torus, in_specs=in_specs, out_specs=out_specs, check_vma=False)
```

```python
import jax
import jax.numpy as jnp
from jax import lax
from jax.experimental import pallas as pl
from jax.experimental.pallas import tpu as pltpu
from jax.sharding import Mesh
from jax.sharding import PartitionSpec as P

KEY_DIM = 64
SP = ("sp_0", "sp_1")
SP_TP = ("sp_0", "sp_1", "tp_0", "tp_1")
TP = ("tp_0", "tp_1")
LANES = 128
COPY_ROWS = 256
ISSUED = (3, 5, 7, 8, 8)
PLAN = (256, 512, 512, 512, 256)
SEQ_ROWS = 16
ENDS_AT = 32
F32 = jnp.float32
BF16 = jnp.bfloat16


def lane_iota(shape):
    return lax.broadcasted_iota(jnp.int32, shape, len(shape) - 1)


def row_iota(shape):
    return lax.broadcasted_iota(jnp.int32, shape, 0)


def log_sigmoid(x):
    return jnp.minimum(x, 0.0) - jnp.log1p(jnp.exp(-jnp.abs(x)))


def key_activation(mixed):
    return (mixed * jax.nn.sigmoid(mixed) * KEY_DIM ** (-0.5)).astype(BF16)


def split(x):
    high = x.astype(BF16).astype(F32)
    middle = (x - high).astype(BF16).astype(F32)
    return [high, middle, x - high - middle]


def suffix_after(x):
    length = x.shape[-1]
    lanes = lane_iota(x.shape)

    def ahead(y, by):
        return jnp.where(lanes < length - by, pltpu.roll(y, length - by, y.ndim - 1), 0.0)

    total = ahead(x, 1)
    by = 1
    while by < length:
        total = total + ahead(total, by)
        by *= 2
    return total


def state_kernel(
    x_hbm, wk_hbm, wv_hbm, wi_hbm, wf_hbm, bias_hbm, taps_hbm, extra_hbm, out_ref,
    x_ref, w_ref, wi_ref, wf_ref, bias_ref, taps_ref, extra_ref, spread_ref, raw_ref, gate_ref, value_ref,
    x_sem, w_sem, small_sem,
):
    seqs, _, rows = extra_ref.shape
    total_rows, width = x_ref.shape
    owners = LANES // 8
    half = lane_iota((1, LANES)) < KEY_DIM

    small = [
        pltpu.make_async_copy(src, dst, small_sem.at[i])
        for i, (src, dst) in enumerate(
            [(wi_hbm, wi_ref), (wf_hbm, wf_ref), (bias_hbm, bias_ref), (taps_hbm, taps_ref), (extra_hbm, extra_ref)]
        )
    ]
    weights = [
        pltpu.make_async_copy(wk_hbm, w_ref.at[:, 0:LANES], w_sem.at[0]),
        pltpu.make_async_copy(wv_hbm, w_ref.at[:, 2 * LANES : 4 * LANES], w_sem.at[1]),
    ]
    blocks = [
        pltpu.make_async_copy(x_hbm.at[pl.ds(at, COPY_ROWS)], x_ref.at[pl.ds(at, COPY_ROWS)], x_sem.at[at // COPY_ROWS])
        for at in range(0, total_rows, COPY_ROWS)
    ]
    for copy in small + weights[:1] + blocks[:1]:
        copy.start()
    for copy in small:
        copy.wait()

    pad = jnp.zeros((6, LANES), F32)
    tail = jnp.zeros((LANES - 16, LANES), F32)
    for c in range(width // LANES):
        cols = slice(c * LANES, (c + 1) * LANES)
        gates = jnp.concatenate([wi_ref[:, cols].astype(F32), pad, wf_ref[:, cols].astype(F32), pad, tail], axis=0)
        w_ref[cols, LANES : 2 * LANES] = gates.T.astype(BF16)
    spot = lax.broadcasted_iota(jnp.int32, spread_ref.shape, 0)
    goal = (spot // LANES) * 8 + spot % 8
    spread_ref[...] = jnp.where(goal == lane_iota(spread_ref.shape), 1.0, 0.0).astype(BF16)
    taps = taps_ref[...].astype(F32)
    bias = jnp.where(row_iota((2, 1)) == 0, bias_ref[:, 0:1], bias_ref[:, 1:2])
    weights[0].wait()
    weights[1].start()

    def project(start, count):
        at = slice(start, start + count)
        key_gate = jnp.dot(x_ref[at], w_ref[:, : 2 * LANES], preferred_element_type=F32)
        if start == 0:
            weights[1].wait()
        value = jnp.dot(x_ref[at], w_ref[:, 2 * LANES :], preferred_element_type=F32)
        raw_ref[at] = key_gate[:, :LANES].astype(BF16)
        gate_ref[at] = key_gate[:, LANES:]
        value_ref[at] = value.astype(BF16)

    def prepare(s):
        own = slice(s * rows, (s + 1) * rows)
        values = value_ref[own]
        raw = raw_ref[own].astype(F32)
        gates = gate_ref[own].T
        input_pre = gates[0:2].astype(BF16).astype(F32)
        forget_pre = gates[8:10].astype(BF16).astype(F32)
        log_forget = log_sigmoid(forget_pre + bias) + extra_ref[s]
        gate_log = input_pre + suffix_after(log_forget)
        peak = jnp.max(gate_log, axis=1, keepdims=True)
        seg_total = jnp.sum(log_forget, axis=1, keepdims=True)
        scale = jnp.exp(gate_log - peak)

        before = pltpu.roll(raw, 1, 0)
        after = pltpu.roll(raw, rows - 1, 0)
        mixed = taps[0:1] * before + taps[1:2] * raw + taps[2:3] * after
        place = row_iota((rows, 1))
        inner = (place > 0) & (place < rows - 1)
        key_rows = jnp.where(inner, key_activation(mixed).astype(F32), 0.0)
        key_t = key_rows.T
        scaled_t = jnp.concatenate([key_t[:KEY_DIM] * scale[0:1], key_t[KEY_DIM:] * scale[1:2]], axis=0)
        scale_parts = split(scale)
        pieces = jnp.concatenate(scale_parts + [jnp.zeros_like(scale)], axis=0).astype(BF16)
        ends = []
        for at in (0, rows - 1):
            for h in range(2):
                row = values[at : at + 1, h * LANES : (h + 1) * LANES].astype(F32)
                ends.append(row * scale[h : h + 1, at : at + 1])
        ends = jnp.concatenate(ends, axis=1)
        spot = lax.broadcasted_iota(jnp.int32, (owners, ends.shape[1]), 1)
        mine = (spot % LANES) // 8 == row_iota((owners, 1))
        picked = jnp.where(mine, ends, 0.0).astype(BF16)
        lane = lane_iota((1, LANES))
        ends_row = jnp.zeros((1, LANES), F32)
        stats_row = jnp.zeros((1, LANES), F32)
        for i, part in enumerate(scale_parts[:2]):
            for p, at in enumerate((0, rows - 1)):
                for h in range(2):
                    ends_row = jnp.where(lane == ENDS_AT + 4 * i + 2 * p + h, part[h : h + 1, at : at + 1], ends_row)
        for i, part in enumerate(split(peak) + split(seg_total)):
            for h in range(2):
                stats_row = jnp.where(lane == 2 * i + h, part[h : h + 1], stats_row)
        raw_rows = jnp.concatenate([raw[0:2], raw[rows - 2 : rows]], axis=0)
        return scaled_t.astype(BF16), pieces, key_rows.astype(BF16), picked, raw_rows, ends_row, stats_row

    def finish(s, prepared):
        scaled_t, pieces, key_rows, picked, raw_rows, ends_row, stats_row = prepared
        values = value_ref[s * rows : (s + 1) * rows]
        memory = jnp.dot(scaled_t, values, preferred_element_type=F32)
        memory = jnp.concatenate([memory[:KEY_DIM, :LANES], memory[KEY_DIM:, LANES:]], axis=0).T
        norm = jnp.dot(pieces, key_rows, preferred_element_type=F32)
        norm = jnp.where(half, norm[0:1] + norm[2:3] + norm[4:5], norm[1:2] + norm[3:4] + norm[5:6])
        by_owner = jnp.dot(picked, spread_ref[...], preferred_element_type=F32)
        shared = jnp.concatenate([raw_rows] + split(norm)[:2] + [ends_row, stats_row], axis=0)
        by_owner = jnp.where(row_iota((8, LANES))[None] == 6, by_owner[:, None, :], 0.0)
        block = jnp.concatenate([memory.reshape(owners, 8, LANES), shared[None] + by_owner], axis=1)
        out_ref[:, s * SEQ_ROWS : (s + 1) * SEQ_ROWS, :] = block.astype(BF16)

    done = 0
    finished = 0
    prepared = {}
    sent = 1
    for step, count in enumerate(PLAN):
        for i in range(done // COPY_ROWS, (done + count) // COPY_ROWS):
            blocks[i].wait()
        for i in range(sent, min(len(blocks), ISSUED[step])):
            blocks[i].start()
        sent = max(sent, ISSUED[step])
        for s in prepared:
            finish(s, prepared[s])
        project(done, count)
        ready = done // rows
        prepared = {s: prepare(s) for s in range(finished, ready)}
        finished = ready
        done += count
    for s in prepared:
        finish(s, prepared[s])
    for s in range(finished, seqs):
        finish(s, prepare(s))


def prompt_states(prompt, key_weight, value_weight, input_gate_t, forget_gate_t, forget_bias, key_taps, extra_t):
    seqs, rows, width = prompt.shape
    owners = LANES // 8
    return pl.pallas_call(
        state_kernel,
        in_specs=[pl.BlockSpec(memory_space=pltpu.HBM)] * 8,
        out_specs=pl.BlockSpec(memory_space=pltpu.VMEM),
        out_shape=pltpu.VMEM((owners, seqs * SEQ_ROWS, LANES), BF16),
        scratch_shapes=[
            pltpu.VMEM((seqs * rows, width), BF16),
            pltpu.VMEM((width, 4 * LANES), BF16),
            pltpu.VMEM(input_gate_t.shape, BF16),
            pltpu.VMEM(forget_gate_t.shape, BF16),
            pltpu.VMEM(forget_bias.shape, F32),
            pltpu.VMEM(key_taps.shape, BF16),
            pltpu.VMEM(extra_t.shape, F32),
            pltpu.VMEM((4 * LANES, LANES), BF16),
            pltpu.VMEM((seqs * rows, LANES), BF16),
            pltpu.VMEM((seqs * rows, LANES), F32),
            pltpu.VMEM((seqs * rows, 2 * LANES), BF16),
            pltpu.SemaphoreType.DMA((seqs * rows // COPY_ROWS,)),
            pltpu.SemaphoreType.DMA((2,)),
            pltpu.SemaphoreType.DMA((5,)),
        ],
        compiler_params=pltpu.CompilerParams(vmem_limit_bytes=60 * 1024 * 1024),
        name="prompt_states",
    )(prompt.reshape(seqs * rows, width), key_weight, value_weight, input_gate_t, forget_gate_t, forget_bias, key_taps, extra_t)


def paired(ref, s):
    rows = ref[s].astype(F32)
    return jnp.concatenate([rows[0:1], rows[1:2]], axis=1)


def read_kernel(
    forget_ref, gate_ref, parts_ref, taps_ref, query_ref, key_ref, value_ref, weight_ref,
    memory_hbm, norm_hbm, peak_hbm, sent_out, memory_out, norm_out, peak_out, sems,
):
    devices = parts_ref.shape[0]
    seqs = query_ref.shape[0]
    half = lane_iota((1, LANES)) < KEY_DIM
    heads = jnp.where(half == (row_iota((2, LANES)) == 0), 1.0, 0.0).astype(BF16)
    device = row_iota((devices, 1))
    lane = lane_iota((devices, LANES))
    at_first = (lane < 16) | ((lane & 2) == 0) & (lane >= ENDS_AT)
    taps = taps_ref[...].astype(F32)
    contract = (((0,), (0,)), ((), ()))
    down = lambda y, by: jnp.where(device < devices - by, pltpu.roll(y, devices - by, 0), 0.0)
    by_head = lambda ref, s: jnp.where(half, ref[0:1, s : s + 1], ref[1:2, s : s + 1])
    own_first = LANES - lax.axis_index(SP) * 4
    memories, norms, levels = [], [], []
    peaks = jnp.zeros((2, seqs), F32)
    for s in range(seqs):
        parts = parts_ref[:, s * SEQ_ROWS : (s + 1) * SEQ_ROWS, :].astype(F32)
        row = lambda r: parts[:, 8 + r, :]
        stats = row(7)

        def joined(first):
            ones = [stats[:, first + 2 * i : first + 2 * i + 1] for i in range(3)]
            twos = [stats[:, first + 2 * i + 1 : first + 2 * i + 2] for i in range(3)]
            return jnp.where(half, ones[0] + ones[1] + ones[2], twos[0] + twos[1] + twos[2])

        later = down(joined(6), 1)
        for by in (1, 2, 4, 8):
            later = later + down(later, by)
        level = joined(0) + later
        peak = jnp.max(level, axis=0, keepdims=True)
        factor = jnp.exp(level - peak)
        before = jnp.where(device > 0, pltpu.roll(row(3), 1, 0), 0.0)
        first = key_activation(taps[0:1] * before + taps[1:2] * row(0) + taps[2:3] * row(1)).astype(F32)
        last = key_activation(taps[0:1] * row(2) + taps[1:2] * row(3) + taps[2:3] * down(row(0), 1)).astype(F32)
        ends = row(6)
        ends_first, ends_last = jnp.where(at_first, ends, 0.0), jnp.where(at_first, 0.0, ends)
        left = jnp.concatenate([ends_first, ends_first, ends_last, ends_last], axis=0).astype(BF16)
        right = jnp.concatenate(split(first * factor)[:2] + split(last * factor)[:2], axis=0).astype(BF16)
        edges = lax.dot_general(left, right, contract, preferred_element_type=F32)
        edge = jnp.where(half, edges[0:8] + edges[16:24], edges[8:16] + edges[24:32])
        scaled = edges[32:33] + edges[34:35] + edges[36:37] + edges[38:39]
        scaled_two = edges[33:34] + edges[35:36] + edges[37:38] + edges[39:40]
        memory = edge + jnp.sum(parts[:, 0:8, :] * factor[:, None, :], axis=0)
        norm = jnp.where(half, scaled, scaled_two) + jnp.sum((row(4) + row(5)) * factor, axis=0, keepdims=True)
        memory_bf = memory.astype(BF16)
        memory_out[s, 0] = memory_bf[:, :KEY_DIM]
        memory_out[s, 1] = memory_bf[:, KEY_DIM:]
        own = pltpu.roll(norm, own_first, 1)
        norm_out[s, 0:1, :] = own[:, 0:4].astype(BF16)
        norm_out[s, 1:2, :] = own[:, KEY_DIM : KEY_DIM + 4].astype(BF16)
        for h in range(2):
            mark = (lane_iota(peaks.shape) == s) & (row_iota(peaks.shape) == h)
            peaks = jnp.where(mark, peak[:, h * KEY_DIM : h * KEY_DIM + 1], peaks)
        memories.append(memory)
        norms.append(norm)
        levels.append(peak)
    peak_out[...] = peaks
    copies = [
        pltpu.make_async_copy(src, dst, sems.at[i])
        for i, (src, dst) in enumerate([(memory_out, memory_hbm), (norm_out, norm_hbm), (peak_out, peak_hbm)])
    ]
    for copy in copies:
        copy.start()

    reads = [jnp.zeros((8, LANES), F32), jnp.zeros((8, LANES), F32)]
    for s, (memory, norm, peak) in enumerate(zip(memories, norms, levels)):
        forget = log_sigmoid(by_head(forget_ref, s))
        gate = by_head(gate_ref, s)
        new_peak = jnp.maximum(forget + peak, gate)
        old_scale = jnp.exp(forget + peak - new_peak)
        new_scale = jnp.exp(gate - new_peak)
        query = paired(query_ref, s)
        new_key = new_scale * paired(key_ref, s)
        new_value = lax.dot_general(value_ref[s], heads, contract, preferred_element_type=F32)
        numer = query * (old_scale * memory + new_key * new_value)
        denom = query * (old_scale * norm + new_key)
        spot = lane_iota((8, LANES))
        for h in range(2):
            side = half if h == 0 else jnp.logical_not(half)
            top = jnp.sum(jnp.where(side, numer, 0.0), axis=1, keepdims=True)
            bottom = jnp.sum(jnp.where(side, denom, 0.0), axis=1, keepdims=True)
            read = top / jnp.maximum(jnp.abs(bottom), 1.0)
            reads[h] = jnp.where((spot & 3) == s, read, reads[h])
    read_rows = jnp.concatenate(reads, axis=0).T[0:8].astype(BF16)
    partial = jnp.dot(read_rows, weight_ref[...], preferred_element_type=F32)
    sub = row_iota((8, LANES))
    block = lane_iota((8, LANES)) // 32
    for m in range(partial.shape[1] // (2 * LANES)):
        low = partial[:, 2 * m * LANES : (2 * m + 1) * LANES]
        high = partial[:, (2 * m + 1) * LANES : (2 * m + 2) * LANES]
        both = jnp.where(sub < 4, low, high)
        out = jnp.zeros_like(both)
        for r in range(4):
            moved = pltpu.roll(both, 32 * r, 1) if r else both
            if r:
                near = pltpu.roll(moved, 8 - r, 0)
                wrap = pltpu.roll(moved, 4 - r, 0)
                moved = jnp.where((sub & 3) + r < 4, near, wrap)
            out = jnp.where(block == (((sub & 3) + r) & 3), moved, out)
        sent_out[8 * m : 8 * m + 8, :] = out
    for copy in copies:
        copy.wait()


def first_read(forget, gate, parts, taps, query, key, value, weight):
    seqs = query.shape[0]
    vmem = pl.BlockSpec(memory_space=pltpu.VMEM)
    hbm = pl.BlockSpec(memory_space=pltpu.HBM)
    devices_all = weight.shape[1] // 32
    memory, norm, peak = (((seqs, 2, 8, KEY_DIM), BF16), ((seqs, 2, 4), BF16), ((2, seqs), F32))
    return pl.pallas_call(
        read_kernel,
        in_specs=[vmem] * 8,
        out_specs=[hbm] * 3 + [vmem],
        out_shape=[
            pltpu.HBM(*memory),
            pltpu.HBM(*norm),
            pltpu.HBM(*peak),
            pltpu.VMEM((devices_all, LANES), F32),
        ],
        scratch_shapes=[pltpu.VMEM(*memory), pltpu.VMEM(*norm), pltpu.VMEM(*peak), pltpu.SemaphoreType.DMA((3,))],
        compiler_params=pltpu.CompilerParams(vmem_limit_bytes=32 * 1024 * 1024),
        name="first_read",
    )(forget, gate, parts, taps, query, key, value, weight)


def sum_kernel(parts_ref, out_ref):
    total = jnp.sum(parts_ref[...], axis=0, keepdims=True)
    for s in range(out_ref.shape[0]):
        out_ref[s : s + 1, :] = total[:, 32 * s : 32 * s + 32].astype(BF16)


def sum_parts(parts, seqs):
    vmem = pl.BlockSpec(memory_space=pltpu.VMEM)
    return pl.pallas_call(
        sum_kernel,
        in_specs=[vmem],
        out_specs=vmem,
        out_shape=jax.ShapeDtypeStruct((seqs, 32), BF16),
        compiler_params=pltpu.CompilerParams(vmem_limit_bytes=1024 * 1024),
        name="sum_parts",
    )(parts)


def body(
    prompt, key_weight, value_weight, input_gate_weight, forget_gate_weight, forget_bias, key_taps,
    extra_decay, new_query, new_key, new_value, new_input_gate, new_forget_gate, out_weight,
):
    seqs = prompt.shape[0]
    parts = prompt_states(
        prompt, key_weight, value_weight, input_gate_weight.T, forget_gate_weight.T, forget_bias.reshape(1, -1),
        key_taps, extra_decay.transpose(0, 2, 1),
    )
    parts = lax.all_to_all(parts, SP, 0, 0, tiled=True)
    memory, norm, peak, sent = first_read(
        new_forget_gate.T, new_input_gate.T, parts, key_taps, new_query, new_key, new_value,
        out_weight.reshape(-1, out_weight.shape[2]),
    )
    got = lax.all_to_all(sent.reshape(-1, 1, LANES), SP_TP, 0, 0, tiled=True)
    read_out = sum_parts(got.reshape(-1, LANES), seqs)
    return memory.swapaxes(2, 3), norm, peak.T, read_out


def solution(mesh):
    torus = Mesh(mesh.devices.reshape(4, 4, 4, 2), ("sp_0", "sp_1", "tp_0", "tp_1"))
    in_specs = (
        P(None, SP, None), P(None, TP), P(None, TP), P(None, TP), P(None, TP), P(TP), P(None, TP),
        P(None, SP, TP), P(None, TP, None), P(None, TP, None), P(None, TP, SP), P(None, TP), P(None, TP),
        P(TP, SP, None),
    )
    out_specs = (P(None, TP, None, SP), P(None, TP, SP), P(None, TP), P(None, SP_TP))
    return jax.shard_map(body, mesh=torus, in_specs=in_specs, out_specs=out_specs, check_vma=False)
```

```python
import jax
import jax.numpy as jnp
from jax import lax
from jax.experimental import pallas as pl
from jax.experimental.pallas import tpu as pltpu
from jax.sharding import Mesh
from jax.sharding import PartitionSpec as P

KEY_DIM = 64
SP = ("sp_0", "sp_1")
SP_TP = ("sp_0", "sp_1", "tp_0", "tp_1")
TP = ("tp_0", "tp_1")
LANES = 128
COPY_ROWS = 256
ISSUED = (3, 5, 7, 8, 8)
PLAN = (256, 512, 512, 512, 256)
SEQ_ROWS = 16
ENDS_AT = 32
F32 = jnp.float32
BF16 = jnp.bfloat16


def lane_iota(shape):
    return lax.broadcasted_iota(jnp.int32, shape, len(shape) - 1)


def row_iota(shape):
    return lax.broadcasted_iota(jnp.int32, shape, 0)


def log_sigmoid(x):
    return jnp.minimum(x, 0.0) - jnp.log1p(jnp.exp(-jnp.abs(x)))


def key_activation(mixed):
    return (mixed * jax.nn.sigmoid(mixed) * KEY_DIM ** (-0.5)).astype(BF16)


def split(x):
    high = x.astype(BF16).astype(F32)
    middle = (x - high).astype(BF16).astype(F32)
    return [high, middle, x - high - middle]


def suffix_after(x):
    length = x.shape[-1]
    lanes = lane_iota(x.shape)

    def ahead(y, by):
        return jnp.where(lanes < length - by, pltpu.roll(y, length - by, y.ndim - 1), 0.0)

    total = ahead(x, 1)
    by = 1
    while by < length:
        total = total + ahead(total, by)
        by *= 2
    return total


def state_kernel(
    x_hbm, wk_hbm, wv_hbm, wi_hbm, wf_hbm, bias_hbm, taps_hbm, extra_hbm, out_ref,
    x_ref, w_ref, wi_ref, wf_ref, bias_ref, taps_ref, extra_ref, spread_ref, raw_ref, gate_ref, value_ref,
    x_sem, w_sem, small_sem,
):
    seqs, _, rows = extra_ref.shape
    total_rows, width = x_ref.shape
    owners = LANES // 8
    half = lane_iota((1, LANES)) < KEY_DIM

    small = [
        pltpu.make_async_copy(src, dst, small_sem.at[i])
        for i, (src, dst) in enumerate(
            [(wi_hbm, wi_ref), (wf_hbm, wf_ref), (bias_hbm, bias_ref), (taps_hbm, taps_ref), (extra_hbm, extra_ref)]
        )
    ]
    weights = [
        pltpu.make_async_copy(wk_hbm, w_ref.at[:, 0:LANES], w_sem.at[0]),
        pltpu.make_async_copy(wv_hbm, w_ref.at[:, 2 * LANES : 4 * LANES], w_sem.at[1]),
    ]
    blocks = [
        pltpu.make_async_copy(x_hbm.at[pl.ds(at, COPY_ROWS)], x_ref.at[pl.ds(at, COPY_ROWS)], x_sem.at[at // COPY_ROWS])
        for at in range(0, total_rows, COPY_ROWS)
    ]
    for copy in small + weights[:1] + blocks[:1]:
        copy.start()
    for copy in small:
        copy.wait()
    weights[1].start()

    pad = jnp.zeros((6, LANES), F32)
    tail = jnp.zeros((LANES - 16, LANES), F32)
    for c in range(width // LANES):
        cols = slice(c * LANES, (c + 1) * LANES)
        gates = jnp.concatenate([wi_ref[:, cols].astype(F32), pad, wf_ref[:, cols].astype(F32), pad, tail], axis=0)
        w_ref[cols, LANES : 2 * LANES] = gates.T.astype(BF16)
    spot = lax.broadcasted_iota(jnp.int32, spread_ref.shape, 0)
    goal = (spot // LANES) * 8 + spot % 8
    spread_ref[...] = jnp.where(goal == lane_iota(spread_ref.shape), 1.0, 0.0).astype(BF16)
    taps = taps_ref[...].astype(F32)
    bias = jnp.where(row_iota((2, 1)) == 0, bias_ref[:, 0:1], bias_ref[:, 1:2])
    weights[0].wait()

    def project(start, count):
        at = slice(start, start + count)
        key_gate = jnp.dot(x_ref[at], w_ref[:, : 2 * LANES], preferred_element_type=F32)
        if start == 0:
            weights[1].wait()
        value = jnp.dot(x_ref[at], w_ref[:, 2 * LANES :], preferred_element_type=F32)
        raw_ref[at] = key_gate[:, :LANES].astype(BF16)
        gate_ref[at] = key_gate[:, LANES:]
        value_ref[at] = value.astype(BF16)

    def prepare(s):
        own = slice(s * rows, (s + 1) * rows)
        values = value_ref[own]
        raw = raw_ref[own].astype(F32)
        gates = gate_ref[own].T
        input_pre = gates[0:2].astype(BF16).astype(F32)
        forget_pre = gates[8:10].astype(BF16).astype(F32)
        log_forget = log_sigmoid(forget_pre + bias) + extra_ref[s]
        gate_log = input_pre + suffix_after(log_forget)
        peak = jnp.max(gate_log, axis=1, keepdims=True)
        seg_total = jnp.sum(log_forget, axis=1, keepdims=True)
        scale = jnp.exp(gate_log - peak)

        before = pltpu.roll(raw, 1, 0)
        after = pltpu.roll(raw, rows - 1, 0)
        mixed = taps[0:1] * before + taps[1:2] * raw + taps[2:3] * after
        place = row_iota((rows, 1))
        inner = (place > 0) & (place < rows - 1)
        key_rows = jnp.where(inner, key_activation(mixed).astype(F32), 0.0)
        key_t = key_rows.T
        scaled_t = jnp.concatenate([key_t[:KEY_DIM] * scale[0:1], key_t[KEY_DIM:] * scale[1:2]], axis=0)
        scale_parts = split(scale)
        pieces = jnp.concatenate(scale_parts + [jnp.zeros_like(scale)], axis=0).astype(BF16)
        ends = []
        for at in (0, rows - 1):
            for h in range(2):
                row = values[at : at + 1, h * LANES : (h + 1) * LANES].astype(F32)
                ends.append(row * scale[h : h + 1, at : at + 1])
        ends = jnp.concatenate(ends, axis=1)
        spot = lax.broadcasted_iota(jnp.int32, (owners, ends.shape[1]), 1)
        mine = (spot % LANES) // 8 == row_iota((owners, 1))
        picked = jnp.where(mine, ends, 0.0).astype(BF16)
        lane = lane_iota((1, LANES))
        ends_row = jnp.zeros((1, LANES), F32)
        stats_row = jnp.zeros((1, LANES), F32)
        for i, part in enumerate(scale_parts[:2]):
            for p, at in enumerate((0, rows - 1)):
                for h in range(2):
                    ends_row = jnp.where(lane == ENDS_AT + 4 * i + 2 * p + h, part[h : h + 1, at : at + 1], ends_row)
        for i, part in enumerate(split(peak) + split(seg_total)):
            for h in range(2):
                stats_row = jnp.where(lane == 2 * i + h, part[h : h + 1], stats_row)
        raw_rows = jnp.concatenate([raw[0:2], raw[rows - 2 : rows]], axis=0)
        return scaled_t.astype(BF16), pieces, key_rows.astype(BF16), picked, raw_rows, ends_row, stats_row

    def finish(s, prepared):
        scaled_t, pieces, key_rows, picked, raw_rows, ends_row, stats_row = prepared
        values = value_ref[s * rows : (s + 1) * rows]
        memory = jnp.dot(scaled_t, values, preferred_element_type=F32)
        memory = jnp.concatenate([memory[:KEY_DIM, :LANES], memory[KEY_DIM:, LANES:]], axis=0).T
        norm = jnp.dot(pieces, key_rows, preferred_element_type=F32)
        norm = jnp.where(half, norm[0:1] + norm[2:3] + norm[4:5], norm[1:2] + norm[3:4] + norm[5:6])
        by_owner = jnp.dot(picked, spread_ref[...], preferred_element_type=F32)
        shared = jnp.concatenate([raw_rows] + split(norm)[:2] + [ends_row, stats_row], axis=0)
        by_owner = jnp.where(row_iota((8, LANES))[None] == 6, by_owner[:, None, :], 0.0)
        block = jnp.concatenate([memory.reshape(owners, 8, LANES), shared[None] + by_owner], axis=1)
        out_ref[:, s * SEQ_ROWS : (s + 1) * SEQ_ROWS, :] = block.astype(BF16)

    done = 0
    finished = 0
    prepared = {}
    sent = 1
    for step, count in enumerate(PLAN):
        for i in range(done // COPY_ROWS, (done + count) // COPY_ROWS):
            blocks[i].wait()
        for i in range(sent, min(len(blocks), ISSUED[step])):
            blocks[i].start()
        sent = max(sent, ISSUED[step])
        for s in prepared:
            finish(s, prepared[s])
        project(done, count)
        ready = done // rows
        prepared = {s: prepare(s) for s in range(finished, ready)}
        finished = ready
        done += count
    for s in prepared:
        finish(s, prepared[s])
    for s in range(finished, seqs):
        finish(s, prepare(s))


def prompt_states(prompt, key_weight, value_weight, input_gate_t, forget_gate_t, forget_bias, key_taps, extra_t):
    seqs, rows, width = prompt.shape
    owners = LANES // 8
    return pl.pallas_call(
        state_kernel,
        in_specs=[pl.BlockSpec(memory_space=pltpu.HBM)] * 8,
        out_specs=pl.BlockSpec(memory_space=pltpu.VMEM),
        out_shape=pltpu.VMEM((owners, seqs * SEQ_ROWS, LANES), BF16),
        scratch_shapes=[
            pltpu.VMEM((seqs * rows, width), BF16),
            pltpu.VMEM((width, 4 * LANES), BF16),
            pltpu.VMEM(input_gate_t.shape, BF16),
            pltpu.VMEM(forget_gate_t.shape, BF16),
            pltpu.VMEM(forget_bias.shape, F32),
            pltpu.VMEM(key_taps.shape, BF16),
            pltpu.VMEM(extra_t.shape, F32),
            pltpu.VMEM((4 * LANES, LANES), BF16),
            pltpu.VMEM((seqs * rows, LANES), BF16),
            pltpu.VMEM((seqs * rows, LANES), F32),
            pltpu.VMEM((seqs * rows, 2 * LANES), BF16),
            pltpu.SemaphoreType.DMA((seqs * rows // COPY_ROWS,)),
            pltpu.SemaphoreType.DMA((2,)),
            pltpu.SemaphoreType.DMA((5,)),
        ],
        compiler_params=pltpu.CompilerParams(vmem_limit_bytes=60 * 1024 * 1024),
        name="prompt_states",
    )(prompt.reshape(seqs * rows, width), key_weight, value_weight, input_gate_t, forget_gate_t, forget_bias, key_taps, extra_t)


def paired(ref, s):
    rows = ref[s].astype(F32)
    return jnp.concatenate([rows[0:1], rows[1:2]], axis=1)


def read_kernel(
    forget_ref, gate_ref, parts_ref, taps_ref, query_ref, key_ref, value_ref, weight_ref,
    memory_hbm, norm_hbm, peak_hbm, sent_out, memory_out, norm_out, peak_out, sems,
):
    devices = parts_ref.shape[0]
    seqs = query_ref.shape[0]
    half = lane_iota((1, LANES)) < KEY_DIM
    heads = jnp.where(half == (row_iota((2, LANES)) == 0), 1.0, 0.0).astype(BF16)
    device = row_iota((devices, 1))
    lane = lane_iota((devices, LANES))
    at_first = (lane < 16) | ((lane & 2) == 0) & (lane >= ENDS_AT)
    taps = taps_ref[...].astype(F32)
    contract = (((0,), (0,)), ((), ()))
    down = lambda y, by: jnp.where(device < devices - by, pltpu.roll(y, devices - by, 0), 0.0)
    by_head = lambda ref, s: jnp.where(half, ref[0:1, s : s + 1], ref[1:2, s : s + 1])
    own_first = LANES - lax.axis_index(SP) * 4
    memories, norms, levels = [], [], []
    peaks = jnp.zeros((2, seqs), F32)
    for s in range(seqs):
        parts = parts_ref[:, s * SEQ_ROWS : (s + 1) * SEQ_ROWS, :].astype(F32)
        row = lambda r: parts[:, 8 + r, :]
        stats = row(7)

        def joined(first):
            ones = [stats[:, first + 2 * i : first + 2 * i + 1] for i in range(3)]
            twos = [stats[:, first + 2 * i + 1 : first + 2 * i + 2] for i in range(3)]
            return jnp.where(half, ones[0] + ones[1] + ones[2], twos[0] + twos[1] + twos[2])

        later = down(joined(6), 1)
        for by in (1, 2, 4, 8):
            later = later + down(later, by)
        level = joined(0) + later
        peak = jnp.max(level, axis=0, keepdims=True)
        factor = jnp.exp(level - peak)
        before = jnp.where(device > 0, pltpu.roll(row(3), 1, 0), 0.0)
        first = key_activation(taps[0:1] * before + taps[1:2] * row(0) + taps[2:3] * row(1)).astype(F32)
        last = key_activation(taps[0:1] * row(2) + taps[1:2] * row(3) + taps[2:3] * down(row(0), 1)).astype(F32)
        ends = row(6)
        ends_first, ends_last = jnp.where(at_first, ends, 0.0), jnp.where(at_first, 0.0, ends)
        left = jnp.concatenate([ends_first, ends_first, ends_last, ends_last], axis=0).astype(BF16)
        right = jnp.concatenate(split(first * factor)[:2] + split(last * factor)[:2], axis=0).astype(BF16)
        edges = lax.dot_general(left, right, contract, preferred_element_type=F32)
        edge = jnp.where(half, edges[0:8] + edges[16:24], edges[8:16] + edges[24:32])
        scaled = edges[32:33] + edges[34:35] + edges[36:37] + edges[38:39]
        scaled_two = edges[33:34] + edges[35:36] + edges[37:38] + edges[39:40]
        memory = edge + jnp.sum(parts[:, 0:8, :] * factor[:, None, :], axis=0)
        norm = jnp.where(half, scaled, scaled_two) + jnp.sum((row(4) + row(5)) * factor, axis=0, keepdims=True)
        memory_bf = memory.astype(BF16)
        memory_out[s, 0] = memory_bf[:, :KEY_DIM]
        memory_out[s, 1] = memory_bf[:, KEY_DIM:]
        own = pltpu.roll(norm, own_first, 1)
        norm_out[s, 0:1, :] = own[:, 0:4].astype(BF16)
        norm_out[s, 1:2, :] = own[:, KEY_DIM : KEY_DIM + 4].astype(BF16)
        for h in range(2):
            mark = (lane_iota(peaks.shape) == s) & (row_iota(peaks.shape) == h)
            peaks = jnp.where(mark, peak[:, h * KEY_DIM : h * KEY_DIM + 1], peaks)
        memories.append(memory)
        norms.append(norm)
        levels.append(peak)
    peak_out[...] = peaks
    copies = [
        pltpu.make_async_copy(src, dst, sems.at[i])
        for i, (src, dst) in enumerate([(memory_out, memory_hbm), (norm_out, norm_hbm), (peak_out, peak_hbm)])
    ]
    for copy in copies:
        copy.start()

    reads = [jnp.zeros((8, LANES), F32), jnp.zeros((8, LANES), F32)]
    for s, (memory, norm, peak) in enumerate(zip(memories, norms, levels)):
        forget = log_sigmoid(by_head(forget_ref, s))
        gate = by_head(gate_ref, s)
        new_peak = jnp.maximum(forget + peak, gate)
        old_scale = jnp.exp(forget + peak - new_peak)
        new_scale = jnp.exp(gate - new_peak)
        query = paired(query_ref, s)
        new_key = new_scale * paired(key_ref, s)
        new_value = lax.dot_general(value_ref[s], heads, contract, preferred_element_type=F32)
        numer = query * (old_scale * memory + new_key * new_value)
        denom = query * (old_scale * norm + new_key)
        spot = lane_iota((8, LANES))
        for h in range(2):
            side = half if h == 0 else jnp.logical_not(half)
            top = jnp.sum(jnp.where(side, numer, 0.0), axis=1, keepdims=True)
            bottom = jnp.sum(jnp.where(side, denom, 0.0), axis=1, keepdims=True)
            read = top / jnp.maximum(jnp.abs(bottom), 1.0)
            reads[h] = jnp.where((spot & 3) == s, read, reads[h])
    read_rows = jnp.concatenate(reads, axis=0).T[0:8].astype(BF16)
    partial = jnp.dot(read_rows, weight_ref[...], preferred_element_type=F32)
    sub = row_iota((8, LANES))
    block = lane_iota((8, LANES)) // 32
    for m in range(partial.shape[1] // (2 * LANES)):
        low = partial[:, 2 * m * LANES : (2 * m + 1) * LANES]
        high = partial[:, (2 * m + 1) * LANES : (2 * m + 2) * LANES]
        both = jnp.where(sub < 4, low, high)
        out = jnp.zeros_like(both)
        for r in range(4):
            moved = pltpu.roll(both, 32 * r, 1) if r else both
            if r:
                near = pltpu.roll(moved, 8 - r, 0)
                wrap = pltpu.roll(moved, 4 - r, 0)
                moved = jnp.where((sub & 3) + r < 4, near, wrap)
            out = jnp.where(block == (((sub & 3) + r) & 3), moved, out)
        sent_out[8 * m : 8 * m + 8, :] = out
    for copy in copies:
        copy.wait()


def first_read(forget, gate, parts, taps, query, key, value, weight):
    seqs = query.shape[0]
    vmem = pl.BlockSpec(memory_space=pltpu.VMEM)
    hbm = pl.BlockSpec(memory_space=pltpu.HBM)
    devices_all = weight.shape[1] // 32
    memory, norm, peak = (((seqs, 2, 8, KEY_DIM), BF16), ((seqs, 2, 4), BF16), ((2, seqs), F32))
    return pl.pallas_call(
        read_kernel,
        in_specs=[vmem] * 8,
        out_specs=[hbm] * 3 + [vmem],
        out_shape=[
            pltpu.HBM(*memory),
            pltpu.HBM(*norm),
            pltpu.HBM(*peak),
            pltpu.VMEM((devices_all, LANES), F32),
        ],
        scratch_shapes=[pltpu.VMEM(*memory), pltpu.VMEM(*norm), pltpu.VMEM(*peak), pltpu.SemaphoreType.DMA((3,))],
        compiler_params=pltpu.CompilerParams(vmem_limit_bytes=32 * 1024 * 1024),
        name="first_read",
    )(forget, gate, parts, taps, query, key, value, weight)


def sum_kernel(parts_ref, out_ref):
    total = jnp.sum(parts_ref[...], axis=0, keepdims=True)
    for s in range(out_ref.shape[0]):
        out_ref[s : s + 1, :] = total[:, 32 * s : 32 * s + 32].astype(BF16)


def sum_parts(parts, seqs):
    vmem = pl.BlockSpec(memory_space=pltpu.VMEM)
    return pl.pallas_call(
        sum_kernel,
        in_specs=[vmem],
        out_specs=vmem,
        out_shape=jax.ShapeDtypeStruct((seqs, 32), BF16),
        compiler_params=pltpu.CompilerParams(vmem_limit_bytes=1024 * 1024),
        name="sum_parts",
    )(parts)


def body(
    prompt, key_weight, value_weight, input_gate_weight, forget_gate_weight, forget_bias, key_taps,
    extra_decay, new_query, new_key, new_value, new_input_gate, new_forget_gate, out_weight,
):
    seqs = prompt.shape[0]
    parts = prompt_states(
        prompt, key_weight, value_weight, input_gate_weight.T, forget_gate_weight.T, forget_bias.reshape(1, -1),
        key_taps, extra_decay.transpose(0, 2, 1),
    )
    parts = lax.all_to_all(parts, SP, 0, 0, tiled=True)
    memory, norm, peak, sent = first_read(
        new_forget_gate.T, new_input_gate.T, parts, key_taps, new_query, new_key, new_value,
        out_weight.reshape(-1, out_weight.shape[2]),
    )
    got = lax.all_to_all(sent.reshape(-1, 1, LANES), SP_TP, 0, 0, tiled=True)
    read_out = sum_parts(got.reshape(-1, LANES), seqs)
    return memory.swapaxes(2, 3), norm, peak.T, read_out


def solution(mesh):
    torus = Mesh(mesh.devices.reshape(4, 4, 4, 2), ("sp_0", "sp_1", "tp_0", "tp_1"))
    in_specs = (
        P(None, SP, None), P(None, TP), P(None, TP), P(None, TP), P(None, TP), P(TP), P(None, TP),
        P(None, SP, TP), P(None, TP, None), P(None, TP, None), P(None, TP, SP), P(None, TP), P(None, TP),
        P(TP, SP, None),
    )
    out_specs = (P(None, TP, None, SP), P(None, TP, SP), P(None, TP), P(None, SP_TP))
    return jax.shard_map(body, mesh=torus, in_specs=in_specs, out_specs=out_specs, check_vma=False)
```
